512 devices in a mesh: grp: 2 (over y), sp: 32 (over z), tp: 8 (over x, core).
Axes of the slice: x: 4, y: 2, z: 32, core: 2. Of those that a mesh axis runs over, the one named last changes fastest.
The devices are a block of a 4x8x32 slice.
Arguments:
- tokens: bfloat16 [2048, 8, 2048], P(('sp', 'tp'), 'grp'), parts along dimension 1, may hold values from -6 to 6
- norm_gain: float32 [2048], replicated, may hold values from 0.1 to 1.9
- w_query: bfloat16 [2048, 2048], P('sp', 'tp'), may hold values from -0.125 to 0.125
- w_value: bfloat16 [2048, 2048], P('sp', 'tp'), may hold values from -0.125 to 0.125
- w_fwd_gate: bfloat16 [2048, 2048], P('sp', 'tp'), may hold values from -0.125 to 0.125
- w_bwd_gate: bfloat16 [2048, 2048], P('sp', 'tp'), may hold values from -0.125 to 0.125
- w_out_gate: bfloat16 [2048, 2048], P('sp', 'tp'), may hold values from -0.125 to 0.125
- floor_gap: float32 [2, 2048], P(None, 'tp'), may hold values from 9.765625e-05 to 0.1
- decay_shift: float32 [2048, 8, 2048], P('sp', 'grp', 'tp'), parts along dimension 1, may hold values from -1.1 to 0
- head_gain: float32 [128], replicated, may hold values from 0.1 to 1.9
- w_out: bfloat16 [2048, 2048], P('tp', 'sp'), may hold values from -0.125 to 0.125
Outputs:
- layer_out: bfloat16 [2048, 8, 2048], P(('sp', 'tp'), 'grp'), parts along dimension 1
The draws below stay inside these ranges and needn't reach their ends.
There are 2 independent parts, one for each index of `grp`. The reference program is written for one: setup_inputs(seed, part) draws one part's arguments, and reference() takes and returns one part's arrays. A program takes and returns all parts, laid end to end along the dimension named above; an argument that names none is the same for every part. Nothing has to cross between parts.
All inputs are finite; a program needn't handle non-finite values.
Results may differ from the reference program's by a relative error of at most 0.013.
Values may be sent and summed in bfloat16 or wider, within the bound.
A program may use at most 128 MiB of HBM per device.

```python
import math
import jax
import jax.numpy as jnp
from jax import lax

D = 2048
HEADS = 16
KEY = 128
VAL = 128
SEQS = 4
SPAN = 64
TOKENS = 2048
N_TP = 8


def draw_floor_gap(key, part):
    key_order, key_count, key_slow, key_fast = jax.random.split(key, 4)
    head_ranks = jax.random.permutation(key_order, HEADS)
    slow_count = jax.random.randint(key_count, (), 2, HEADS - 1)
    slow_heads = jnp.repeat(head_ranks < slow_count, KEY)[None, :]
    slow_gap = jnp.exp(jax.random.uniform(key_slow, (2, HEADS * KEY), jnp.float32, math.log(0.2), math.log(0.8))) / TOKENS
    fast_gap = jnp.exp(jax.random.uniform(key_fast, (2, HEADS * KEY), jnp.float32, math.log(0.03), math.log(0.1)))
    return jnp.where(slow_heads, slow_gap, fast_gap).astype(jnp.float32)


def draw_decay_shift(key, part):
    key_block, key_chan, key_place, key_depth = jax.random.split(key, 4)
    block_rate = jnp.exp(jax.random.uniform(key_block, (TOKENS // SPAN, SEQS, 1), jnp.float32, math.log(0.5), math.log(2.0)))
    channel_rate = jnp.exp(jax.random.uniform(key_chan, (1, 1, HEADS * KEY), jnp.float32, math.log(0.3), 0.0))
    stable_regime = -(0.5 / TOKENS) * jnp.repeat(block_rate, SPAN, axis=0) * channel_rate
    seat_indices = jax.random.randint(key_place, (2, SEQS), 0, TOKENS)
    layer_tiers = jax.random.uniform(key_depth, (2, SEQS), jnp.float32, math.log(0.6), math.log(0.8))
    location_indices = jnp.arange(TOKENS)[:, None]
    cluster_tally = jnp.where(location_indices == seat_indices[0][None, :], layer_tiers[0][None, :], 0.0)
    cluster_tally = cluster_tally + jnp.where(location_indices == seat_indices[1][None, :], layer_tiers[1][None, :], 0.0)
    return (stable_regime + cluster_tally[:, :, None]).astype(jnp.float32)


def steps_of(key, extent, cuts, least, top_value):
    factor_of, own = 1.0, jax.random.fold_in(key, 6)
    for position, parts in cuts:
        draws = jnp.exp(jax.random.uniform(jax.random.fold_in(own, position), (parts,), jnp.float32, least / len(cuts), top_value / len(cuts)))
        factor_of = factor_of * jnp.repeat(draws, extent[position] // parts).reshape([-1 if axis == position else 1 for axis in range(len(extent))])
    return factor_of


def gaussian(stream_key, extent, deviation, reach, cuts=(), dtype=jnp.bfloat16):
    level = steps_of(stream_key, extent, cuts, -0.22, 0.18) if cuts else 1.0
    entries = jax.random.normal(stream_key, extent, jnp.float32) * deviation * level
    return jnp.minimum(jnp.maximum(entries, -reach), reach).astype(dtype)


def setup_inputs(seed: int = 0, part: int = 0) -> dict:
    splits = jax.random.split(jax.random.key(seed), 12)
    part_splits = jax.random.split(jax.random.fold_in(splits[11], part), 12)
    tokens = gaussian(part_splits[0], (TOKENS, SEQS, D), 1.0, 6.0, ((0, 256),))
    norm_gain = jnp.clip(1.0 + 0.18 * jax.random.normal(splits[1], (D,), jnp.float32), 0.1, 1.9)
    w_query = gaussian(splits[2], (D, HEADS * KEY), D ** -0.5, 0.125, ((0, 32), (1, 8)))
    w_value = gaussian(splits[3], (D, HEADS * VAL), D ** -0.5, 0.125, ((0, 32), (1, 8)))
    w_fwd_gate = gaussian(splits[4], (D, HEADS * KEY), D ** -0.5, 0.125, ((0, 32), (1, 8)))
    w_bwd_gate = gaussian(splits[5], (D, HEADS * KEY), D ** -0.5, 0.125, ((0, 32), (1, 8)))
    w_out_gate = gaussian(splits[6], (D, HEADS * VAL), D ** -0.5, 0.125, ((0, 32), (1, 8)))
    floor_gap = draw_floor_gap(jax.random.fold_in(splits[11], 71), part)
    decay_shift = draw_decay_shift(jax.random.fold_in(jax.random.fold_in(splits[11], part), 71), part)
    head_gain = jnp.clip(1.0 + 0.18 * jax.random.normal(splits[9], (VAL,), jnp.float32), 0.1, 1.9)
    w_out = gaussian(splits[10], (HEADS * VAL, D), (HEADS * VAL) ** -0.5, 0.125, ((0, 8), (1, 32)))
    return {"tokens": tokens, "norm_gain": norm_gain, "w_query": w_query, "w_value": w_value, "w_fwd_gate": w_fwd_gate, "w_bwd_gate": w_bwd_gate, "w_out_gate": w_out_gate, "floor_gap": floor_gap, "decay_shift": decay_shift, "head_gain": head_gain, "w_out": w_out}


norm_eps = 1e-06
highest = lax.Precision.HIGHEST

def chain_scan(queries, key_cols, values, log_decay, backward):

    def advance(carry_state, inputs):
        query_now, key_now, value_now, decay_now = inputs
        carry_state = jnp.exp(decay_now)[..., None] * carry_state + key_now[..., None] * value_now[..., None, :]
        return (carry_state, jnp.einsum('bhk,bhke->bhe', query_now, carry_state, precision=highest))
    start_state = jnp.zeros((SEQS, HEADS, KEY, VAL), jnp.float32)
    _, outputs = lax.scan(advance, start_state, (queries, key_cols, values, log_decay), reverse=backward)
    return outputs

def reference(tokens, norm_gain, w_query, w_value, w_fwd_gate, w_bwd_gate, w_out_gate, floor_gap, decay_shift, head_gain, w_out):
    token_f32 = tokens.astype(jnp.float32)
    scale_rows = lax.rsqrt(lax.optimization_barrier(jnp.mean(token_f32 * token_f32, axis=-1, keepdims=True)) + norm_eps)
    normed = (token_f32 * scale_rows * norm_gain.astype(jnp.float32)).astype(jnp.bfloat16)
    flat_rows = normed.reshape(TOKENS * SEQS, D)

    def project(matrix):
        rounded = jnp.dot(flat_rows, matrix, preferred_element_type=jnp.float32).astype(jnp.bfloat16)
        return lax.optimization_barrier(rounded).astype(jnp.float32)
    queries = jax.nn.silu(project(w_query)).reshape(TOKENS, SEQS, HEADS, KEY)
    values = project(w_value).reshape(TOKENS, SEQS, HEADS, VAL)
    shift = decay_shift.reshape(TOKENS, SEQS, HEADS, KEY)
    gap_fwd = floor_gap[0].reshape(HEADS, KEY)
    gap_bwd = floor_gap[1].reshape(HEADS, KEY)
    key_fwd = gap_fwd * jax.nn.sigmoid(-project(w_fwd_gate).reshape(TOKENS, SEQS, HEADS, KEY))
    key_bwd = gap_bwd * jax.nn.sigmoid(-project(w_bwd_gate).reshape(TOKENS, SEQS, HEADS, KEY))
    decay_fwd = jnp.log1p(-key_fwd) + shift
    decay_bwd = jnp.log1p(-key_bwd) + shift
    combined = chain_scan(queries, key_fwd, values, decay_fwd, False) + chain_scan(queries, key_bwd, values, decay_bwd, True)
    head_normed = combined * lax.rsqrt(lax.optimization_barrier(jnp.mean(combined * combined, axis=-1, keepdims=True)) + norm_eps) * head_gain.astype(jnp.float32)
    gate_value = jax.nn.silu(project(w_out_gate))
    mixed = (head_normed.reshape(TOKENS * SEQS, HEADS * VAL) * gate_value).astype(jnp.bfloat16)
    group_width = HEADS * VAL // N_TP
    accumulated_total = jnp.zeros((TOKENS * SEQS, D), jnp.float32)
    for tp_group in range(N_TP):
        first_column = tp_group * group_width
        partial_value = jnp.dot(mixed[:, first_column:first_column + group_width], w_out[first_column:first_column + group_width], preferred_element_type=jnp.float32).astype(jnp.bfloat16)
        accumulated_total = accumulated_total + lax.optimization_barrier(partial_value).astype(jnp.float32)
    return accumulated_total.astype(jnp.bfloat16).reshape(TOKENS, SEQS, D)
```

```python
import functools

import jax
import jax.numpy as jnp
from jax import lax
from jax.experimental import pallas as pl
from jax.experimental.pallas import tpu as pltpu
from jax.sharding import PartitionSpec as P

MESH = pl.DeviceIdType.MESH
F32 = jnp.float32
BF16 = jnp.bfloat16
CH = 128
BLK = 4
SLOTS = 4
EPS = 1e-06


def dims(contract):
    return (contract, ((), ()))


def kernel(
    n_sp,
    n_tp,
    tokens,
    gain,
    w_query,
    w_value,
    w_fwd,
    w_bwd,
    w_gate,
    w_out,
    gap,
    shift,
    head_gain,
    out,
    weights,
    normed,
    qs,
    vs,
    kf,
    kb,
    rf,
    rb,
    gs,
    qe,
    inner,
    local,
    decay,
    before,
    decay_before,
    sent1,
    decay_sent,
    total,
    ahead,
    sent2,
    carried,
    mixed,
    mine,
    given,
    taken,
    summed,
    pieces,
    ring_send,
    ring_recv,
    y_send,
    y_recv,
    tok_send,
    tok_recv,
    d_send,
    d_recv,
    p1_send,
    p1_recv,
    p2_send,
    p2_recv,
    pair_send,
    pair_recv,
    x_send,
    x_recv,
):
    z = lax.axis_index("sp")
    tp = lax.axis_index("tp")
    grp = lax.axis_index("grp")
    parity = lax.rem(grp, 2)
    mate = grp + 1 - 2 * parity
    right, left = lax.rem(z + 1, n_sp), lax.rem(z + n_sp - 1, n_sp)
    n_x = n_tp // 2
    core, x = lax.rem(tp, 2), tp // 2
    wrows, width = w_query.shape
    step_pos, seqs, model = tokens.shape
    span = shift.shape[0]
    heads = width // CH
    chunks = seqs * heads
    n_blocks = n_sp // BLK
    block_rows = step_pos * seqs
    half = n_sp // 2

    def spot(t):
        return (t % 2) * n_x + t // 2

    here = spot(tp)

    own_rows = pl.ds(pl.multiple_of(z * wrows, wrows), wrows)
    for m, ref in enumerate((w_value, w_fwd, w_bwd, w_gate, w_query)):
        weights[m, own_rows, :] = ref[...]
    eye = (
        lax.broadcasted_iota(jnp.int32, (width, width), 0)
        == lax.broadcasted_iota(jnp.int32, (width, width), 1)
    ).astype(F32).astype(BF16)
    weights[5, own_rows, :] = lax.dot_general(
        w_out[...], eye, dims(((0,), (0,))), preferred_element_type=F32
    ).astype(BF16)

    barrier = pltpu.get_barrier_semaphore()
    greeted = 0
    for peer in (
        [{"sp": right}, {"sp": left}]
        + [{"sp": lax.rem(z + BLK, n_sp)}, {"sp": lax.rem(z + n_sp - BLK, n_sp)}]
        + [{"tp": lax.rem(tp + d, n_tp)} for d in range(1, n_tp)]
        + [{"grp": mate}]
    ):
        pl.semaphore_signal(barrier, inc=1, device_id=peer, device_id_type=MESH)
        greeted += 1
    pl.semaphore_wait(barrier, greeted)

    def matrix(slot, par):
        return slot if slot < 2 else slot + 2 * par

    def block(slot, origin, par):
        return weights.at[
            matrix(slot, par), pl.ds(pl.multiple_of(origin * wrows, wrows), wrows)
        ]

    def hop(slot, origin, step, way):
        ref = block(slot, origin, parity)
        return pltpu.make_async_remote_copy(
            src_ref=ref,
            dst_ref=ref,
            send_sem=ring_send.at[way, slot],
            recv_sem=ring_recv.at[way, slot, step],
            device_id={"sp": left if way else right},
            device_id_type=MESH,
        )

    def over(ref, k):
        return pltpu.make_async_remote_copy(
            src_ref=ref,
            dst_ref=ref,
            send_sem=y_send.at[k],
            recv_sem=y_recv.at[k],
            device_id={"grp": mate},
            device_id_type=MESH,
        )

    for slot in range(SLOTS):
        for way in (0, 1):
            hop(slot, z, 1, way).start()

    tok = tokens[...].astype(F32)
    rows = []
    for b in range(seqs):
        part = tok[:, b, :]
        scale = lax.rsqrt(jnp.mean(part * part, axis=-1, keepdims=True) + EPS)
        rows.append(part * scale * gain[...])
    tok_block = pl.ds(pl.multiple_of(here * block_rows, block_rows), block_rows)
    normed[tok_block, :] = jnp.concatenate(rows, axis=0).astype(BF16)

    def token_copy(ref, peer):
        return pltpu.make_async_remote_copy(
            src_ref=ref,
            dst_ref=ref,
            send_sem=tok_send,
            recv_sem=tok_recv,
            device_id={"tp": peer},
            device_id_type=MESH,
        )

    for d in range(1, n_tp):
        token_copy(normed.at[tok_block], lax.rem(tp + d, n_tp)).start()

    def arrive(slot, step, way, forward):
        origin = lax.rem(z + step, n_sp) if way else lax.rem(z + n_sp - step, n_sp)
        hop(slot, origin, step, way).wait_recv()
        if forward is True:
            hop(slot, origin, step + 1, way).start()
        elif forward is not False:
            @pl.when(forward)
            def _():
                hop(slot, origin, step + 1, way).start()
        if slot >= 2:
            over(block(slot, origin, parity), slot - 2).start()

    def ring_step(step, carry):
        for slot in range(SLOTS):
            arrive(slot, step, 0, True)
            arrive(slot, step, 1, step < half - 1)
        return carry

    lax.fori_loop(1, half, ring_step, 0)
    for slot in range(SLOTS):
        arrive(slot, half, 0, False)

    others = block_rows * (n_tp - 1)
    token_copy(normed.at[pl.ds(0, others)], tp).wait_recv()

    def project(m):
        return (
            jnp.dot(normed[...], weights[m], preferred_element_type=F32)
            .astype(BF16)
            .astype(F32)
        )

    def by_sequence(ref, value):
        for t in range(n_tp):
            for b in range(seqs):
                first = spot(t) * block_rows + b * step_pos
                ref[b, t * step_pos : (t + 1) * step_pos, :] = value[
                    first : first + step_pos, :
                ]

    def silu(u):
        return u / (1.0 + jnp.exp(-u))

    by_sequence(vs, project(0))
    by_sequence(kf, gap[0:1, :] / (1.0 + jnp.exp(project(1))))
    for k in range(2):
        theirs = weights.at[2 + k + 2 * (1 - parity), pl.ds(0, wrows * (n_sp - 1))]
        over(theirs, k).wait_recv()
    by_sequence(kb, gap[1:2, :] / (1.0 + jnp.exp(project(2))))

    at_row = lax.broadcasted_iota(jnp.int32, (span, span), 0)
    at_col = lax.broadcasted_iota(jnp.int32, (span, span), 1)
    lower = (at_row >= at_col).astype(F32)
    upper = (at_row <= at_col).astype(F32)
    for b in range(seqs):
        moved = shift[:, b, :]
        fwd_key, bwd_key = kf[b], kb[b]
        fwd_run = jnp.dot(
            lower,
            jnp.log1p(-fwd_key) + moved,
            precision=lax.Precision.HIGHEST,
            preferred_element_type=F32,
        )
        bwd_run = jnp.dot(
            upper,
            jnp.log1p(-bwd_key) + moved,
            precision=lax.Precision.HIGHEST,
            preferred_element_type=F32,
        )
        rf[b] = fwd_run
        rb[b] = bwd_run
        fwd_end, bwd_end = fwd_run[span - 1 : span, :], bwd_run[0:1, :]
        keys = jnp.concatenate(
            [fwd_key * jnp.exp(fwd_end - fwd_run), bwd_key * jnp.exp(bwd_end - bwd_run)],
            axis=1,
        ).astype(BF16)
        states = lax.dot_general(
            vs[b].astype(BF16), keys, dims(((0,), (0,))), preferred_element_type=F32
        )
        for h in range(heads):
            c = b * heads + h
            lanes = slice(h * CH, (h + 1) * CH)
            for d, end in enumerate((fwd_end, bwd_end)):
                local[d, c] = states[lanes, d * width + h * CH : d * width + (h + 1) * CH]
                decay[d, c : c + 1, :] = jnp.exp(end[:, lanes])

    def ends(d):
        place = (n_sp - 1 - z) if d == 1 else z
        return place // BLK, lax.rem(place, BLK), (-1 if d == 1 else 1)

    def scan_copy(src, dst, send, recv, target):
        return pltpu.make_async_remote_copy(
            src_ref=src,
            dst_ref=dst,
            send_sem=send,
            recv_sem=recv,
            device_id={"sp": target},
            device_id_type=MESH,
        )

    def near(d, way, c=None):
        if c is None:
            return scan_copy(
                decay_sent.at[d], decay_before.at[d], d_send.at[d], d_recv.at[d], z + way
            )
        return scan_copy(
            sent1.at[d, c], before.at[d, c], p1_send.at[d], p1_recv.at[d, c], z + way
        )

    def far(d, way, c):
        return scan_copy(
            sent2.at[d, c], ahead.at[d, c], p2_send.at[d, 0], p2_recv.at[d, c], z + BLK * way
        )

    def down(d, way, c):
        return scan_copy(
            sent2.at[d, c], ahead.at[d, c], p2_send.at[d, 1], p2_recv.at[d, c], z + way
        )

    def relay(d, way, c):
        return scan_copy(
            ahead.at[d, c], ahead.at[d, c], p2_send.at[d, 1], p2_recv.at[d, c], z + way
        )

    for d in (0, 1):
        jj, rr, way = ends(d)

        @pl.when(jj == 0)
        def _():
            ahead[d] = jnp.zeros(ahead.shape[1:], ahead.dtype)

        @pl.when(rr == 0)
        def _():
            before[d] = jnp.zeros(before.shape[1:], before.dtype)
            decay_before[d] = jnp.ones(decay_before.shape[1:], F32)

        @pl.when(rr > 0)
        def _():
            near(d, way).wait_recv()

        decay_sent[d] = decay_before[d] * decay[d]

        @pl.when(rr < BLK - 1)
        def _():
            near(d, way).start()

    def first_pass(c, carry):
        for d in (0, 1):
            jj, rr, way = ends(d)

            @pl.when(rr > 0)
            def _():
                near(d, way, c).wait_recv()

            joined = decay[d, pl.ds(c, 1), :] * before[d, c].astype(F32) + local[d, c]

            @pl.when(rr < BLK - 1)
            def _():
                sent1[d, c] = joined.astype(BF16)
                near(d, way, c).start()

            @pl.when(rr == BLK - 1)
            def _():
                total[d, c] = joined

                @pl.when(jj == 0)
                def _():
                    sent2[d, c] = joined.astype(BF16)
                    far(d, way, c).start()
                    down(d, way, c).start()

        return carry

    lax.fori_loop(0, chunks, first_pass, 0)

    def second_pass(d):
        jj, rr, way = ends(d)

        def each(c, carry):
            @pl.when(jj > 0)
            def _():
                far(d, way, c).wait_recv()

            @pl.when((rr == BLK - 1) & (jj > 0) & (jj < n_blocks - 1))
            def _():
                joined = (
                    decay_sent[d, pl.ds(c, 1), :] * ahead[d, c].astype(F32) + total[d, c]
                )
                sent2[d, c] = joined.astype(BF16)
                far(d, way, c).start()
                down(d, way, c).start()

            @pl.when((rr < BLK - 2) & (jj > 0))
            def _():
                relay(d, way, c).start()

            carried[c, :, d * CH : (d + 1) * CH] = (
                decay_before[d, pl.ds(c, 1), :] * ahead[d, c].astype(F32)
                + before[d, c].astype(F32)
            ).astype(BF16)
            return carry

        lax.fori_loop(0, chunks, each, 0)

    def inside():
        by_sequence(qs, silu(project(4)))
        by_sequence(gs, silu(project(3)))
        middle = span // 2 - 1
        for b in range(seqs):
            query, fwd_run, bwd_run = qs[b], rf[b], rb[b]
            fwd_mid, bwd_mid = fwd_run[middle : middle + 1, :], bwd_run[middle : middle + 1, :]
            fwd_q = (query * jnp.exp(fwd_run - fwd_mid)).astype(BF16)
            bwd_q = (query * jnp.exp(bwd_run - bwd_mid)).astype(BF16)
            fwd_k = (kf[b] * jnp.exp(fwd_mid - fwd_run)).astype(BF16)
            bwd_k = (kb[b] * jnp.exp(bwd_mid - bwd_run)).astype(BF16)
            fwd_e = (query * jnp.exp(fwd_run)).astype(BF16)
            bwd_e = (query * jnp.exp(bwd_run)).astype(BF16)
            value = vs[b].astype(BF16)
            for h in range(heads):
                c = b * heads + h
                lanes = slice(h * CH, (h + 1) * CH)
                fwd_s = lax.dot_general(
                    fwd_q[:, lanes], fwd_k[:, lanes], dims(((1,), (1,))), preferred_element_type=F32
                )
                bwd_s = lax.dot_general(
                    bwd_q[:, lanes], bwd_k[:, lanes], dims(((1,), (1,))), preferred_element_type=F32
                )
                scores = jnp.where(at_row >= at_col, fwd_s, 0.0) + jnp.where(
                    at_row <= at_col, bwd_s, 0.0
                )
                inner[c] = jnp.dot(
                    scores.astype(BF16), value[:, lanes], preferred_element_type=F32
                )
                qe[c] = jnp.concatenate([fwd_e[:, lanes], bwd_e[:, lanes]], axis=1)

    low = z < half

    @pl.when(low)
    def _():
        second_pass(0)

    @pl.when(jnp.logical_not(low))
    def _():
        second_pass(1)

    inside()

    @pl.when(low)
    def _():
        second_pass(1)

    @pl.when(jnp.logical_not(low))
    def _():
        second_pass(0)

    for b in range(seqs):
        for h in range(heads):
            c = b * heads + h
            both = inner[c] + lax.dot_general(
                qe[c], carried[c], dims(((1,), (1,))), preferred_element_type=F32
            )
            scale = lax.rsqrt(jnp.mean(both * both, axis=-1, keepdims=True) + EPS)
            gated = both * scale * head_gain[...] * gs[b, :, h * CH : (h + 1) * CH]
            for t in range(n_tp):
                first = spot(t) * block_rows + b * step_pos
                mixed[first : first + step_pos, h * CH : (h + 1) * CH] = gated[
                    t * step_pos : (t + 1) * step_pos, :
                ]

    side = n_x * block_rows

    def partial(which):
        lines = pl.ds(pl.multiple_of(which * side, side), side)
        return lax.dot_general(
            mixed[lines, :].astype(BF16),
            weights[5],
            dims(((1,), (1,))),
            preferred_element_type=F32,
        )

    given[...] = partial(1 - core).astype(BF16)
    pair = pltpu.make_async_remote_copy(
        src_ref=given,
        dst_ref=taken,
        send_sem=pair_send,
        recv_sem=pair_recv,
        device_id={"tp": tp + 1 - 2 * core},
        device_id_type=MESH,
    )
    pair.start()
    mine[...] = partial(core)
    pair.wait_recv()

    def piece(dest, d):
        lines = pl.ds(pl.multiple_of(dest * block_rows, block_rows), block_rows)
        return pltpu.make_async_remote_copy(
            src_ref=summed.at[lines],
            dst_ref=pieces.at[d - 1],
            send_sem=x_send.at[d - 1],
            recv_sem=x_recv.at[d - 1],
            device_id={"tp": dest * 2 + core},
            device_id_type=MESH,
        )

    order = [2, 1, 3] if n_x == 4 else list(range(1, n_x))
    for d in order:
        dest = lax.rem(x + d, n_x)
        lines = pl.ds(pl.multiple_of(dest * block_rows, block_rows), block_rows)
        summed[lines, :] = (mine[lines, :] + taken[lines, :].astype(F32)).astype(BF16)
        piece(dest, d).start()
    own_lines = pl.ds(pl.multiple_of(x * block_rows, block_rows), block_rows)
    result = mine[own_lines, :] + taken[own_lines, :].astype(F32)
    for d in range(1, n_x):
        piece(x, d).wait_recv()
        result = result + pieces[d - 1].astype(F32)
    out[...] = result.astype(BF16)

    for slot in range(SLOTS):
        for way in (0, 1):
            length = wrows * (half - way)
            ref = weights.at[matrix(slot, parity), pl.ds(0, length)]
            pltpu.make_async_remote_copy(
                src_ref=ref,
                dst_ref=ref,
                send_sem=ring_send.at[way, slot],
                recv_sem=ring_recv.at[way, slot, 0],
                device_id={"sp": right},
                device_id_type=MESH,
            ).wait_send()
    for k in range(2):
        over(weights.at[k, pl.ds(0, wrows * (n_sp - 1))], k).wait_send()
    token_copy(normed.at[pl.ds(0, others)], tp).wait_send()
    for d in (0, 1):
        jj, rr, way = ends(d)

        @pl.when(rr < BLK - 1)
        def _():
            near(d, way).wait_send()
            scan_copy(sent1.at[d], before.at[d], p1_send.at[d], p1_recv.at[d, 0], z).wait_send()

        leads = (rr == BLK - 1) & (jj < n_blocks - 1)

        @pl.when(leads)
        def _():
            scan_copy(sent2.at[d], ahead.at[d], p2_send.at[d, 0], p2_recv.at[d, 0], z).wait_send()

        @pl.when(leads | ((rr < BLK - 2) & (jj > 0)))
        def _():
            scan_copy(sent2.at[d], ahead.at[d], p2_send.at[d, 1], p2_recv.at[d, 0], z).wait_send()

    pair.wait_send()
    for d in range(1, n_x):
        piece(lax.rem(x + d, n_x), d).wait_send()


def shards(
    n_sp,
    n_tp,
    tokens,
    norm_gain,
    w_query,
    w_value,
    w_fwd_gate,
    w_bwd_gate,
    w_out_gate,
    floor_gap,
    decay_shift,
    head_gain,
    w_out,
):
    step_pos, seqs, model = tokens.shape
    wrows, width = w_query.shape
    span = decay_shift.shape[0]
    chunks = seqs * (width // CH)
    rows = step_pos * seqs
    all_rows = rows * n_tp
    n_x = n_tp // 2
    f32_rows = pltpu.VMEM((seqs, span, width), F32)
    vmem = pl.BlockSpec(memory_space=pltpu.VMEM)
    dma = pltpu.SemaphoreType.DMA
    result = pl.pallas_call(
        functools.partial(kernel, n_sp, n_tp),
        out_shape=jax.ShapeDtypeStruct((rows, model), BF16),
        in_specs=[vmem] * 11,
        out_specs=vmem,
        scratch_shapes=[
            pltpu.VMEM((6, wrows * n_sp, width), BF16),
            pltpu.VMEM((all_rows, model), BF16),
            f32_rows,
            f32_rows,
            f32_rows,
            f32_rows,
            f32_rows,
            f32_rows,
            f32_rows,
            pltpu.VMEM((chunks, span, 2 * CH), BF16),
            pltpu.VMEM((chunks, span, CH), F32),
            pltpu.VMEM((2, chunks, CH, CH), F32),
            pltpu.VMEM((2, chunks, CH), F32),
            pltpu.VMEM((2, chunks, CH, CH), BF16),
            pltpu.VMEM((2, chunks, CH), F32),
            pltpu.VMEM((2, chunks, CH, CH), BF16),
            pltpu.VMEM((2, chunks, CH), F32),
            pltpu.VMEM((2, chunks, CH, CH), F32),
            pltpu.VMEM((2, chunks, CH, CH), BF16),
            pltpu.VMEM((2, chunks, CH, CH), BF16),
            pltpu.VMEM((chunks, CH, 2 * CH), BF16),
            pltpu.VMEM((all_rows, width), F32),
            pltpu.VMEM((n_x * rows, model), F32),
            pltpu.VMEM((n_x * rows, model), BF16),
            pltpu.VMEM((n_x * rows, model), BF16),
            pltpu.VMEM((n_x * rows, model), BF16),
            pltpu.VMEM((n_x - 1, rows, model), BF16),
            dma((2, SLOTS)),
            dma((2, SLOTS, n_sp // 2 + 1)),
            dma((2,)),
            dma((2,)),
            dma,
            dma,
            dma((2,)),
            dma((2,)),
            dma((2,)),
            dma((2, chunks)),
            dma((2, 2)),
            dma((2, chunks)),
            dma,
            dma,
            dma((n_x - 1,)),
            dma((n_x - 1,)),
        ],
        compiler_params=pltpu.CompilerParams(
            collective_id=0, has_side_effects=True, vmem_limit_bytes=60 * 1024 * 1024
        ),
        name="mixer",
    )(
        tokens,
        norm_gain.reshape(1, -1),
        w_query,
        w_value,
        w_fwd_gate,
        w_bwd_gate,
        w_out_gate,
        w_out,
        floor_gap,
        decay_shift,
        head_gain.reshape(1, -1),
    )
    return result.reshape(seqs, step_pos, model).transpose(1, 0, 2)


def solution(mesh):
    in_specs = (
        P(("sp", "tp"), "grp", None),
        P(),
        P("sp", "tp"),
        P("sp", "tp"),
        P("sp", "tp"),
        P("sp", "tp"),
        P("sp", "tp"),
        P(None, "tp"),
        P("sp", "grp", "tp"),
        P(),
        P("tp", "sp"),
    )
    return jax.shard_map(
        functools.partial(shards, mesh.shape["sp"], mesh.shape["tp"]),
        mesh=mesh,
        in_specs=in_specs,
        out_specs=P(("sp", "tp"), "grp", None),
        check_vma=False,
    )
```

```python
import functools

import jax
import jax.numpy as jnp
from jax import lax
from jax.experimental import pallas as pl
from jax.experimental.pallas import tpu as pltpu
from jax.sharding import PartitionSpec as P

MESH = pl.DeviceIdType.MESH
F32 = jnp.float32
BF16 = jnp.bfloat16
CH = 128
BLK = 4
SLOTS = 4
EPS = 1e-06


def dims(contract):
    return (contract, ((), ()))


def kernel(
    n_sp,
    n_tp,
    tokens,
    gain,
    w_query,
    w_value,
    w_fwd,
    w_bwd,
    w_gate,
    w_out,
    gap,
    shift,
    head_gain,
    out,
    weights,
    normed,
    qs,
    vs,
    kf,
    kb,
    rf,
    rb,
    gs,
    qe,
    inner,
    local,
    decay,
    before,
    decay_in,
    decay_before,
    sent1,
    decay_sent,
    total,
    ahead,
    sent2,
    carried,
    mixed,
    mine,
    given,
    taken,
    summed,
    pieces,
    ring_send,
    ring_recv,
    y_send,
    y_recv,
    tok_send,
    tok_recv,
    d_send,
    d_recv,
    p1_send,
    p1_recv,
    p2_send,
    p2_recv,
    pair_send,
    pair_recv,
    x_send,
    x_recv,
):
    z = lax.axis_index("sp")
    tp = lax.axis_index("tp")
    grp = lax.axis_index("grp")
    parity = lax.rem(grp, 2)
    mate = grp + 1 - 2 * parity
    right, left = lax.rem(z + 1, n_sp), lax.rem(z + n_sp - 1, n_sp)
    n_x = n_tp // 2
    core, x = lax.rem(tp, 2), tp // 2
    wrows, width = w_query.shape
    step_pos, seqs, model = tokens.shape
    span = shift.shape[0]
    heads = width // CH
    chunks = seqs * heads
    n_blocks = n_sp // BLK
    block_rows = step_pos * seqs
    half = n_sp // 2

    def spot(t):
        return (t % 2) * n_x + t // 2

    here = spot(tp)

    own_rows = pl.ds(pl.multiple_of(z * wrows, wrows), wrows)
    for m, ref in enumerate((w_value, w_fwd, w_bwd, w_gate, w_query)):
        weights[m, own_rows, :] = ref[...]
    eye = (
        lax.broadcasted_iota(jnp.int32, (width, width), 0)
        == lax.broadcasted_iota(jnp.int32, (width, width), 1)
    ).astype(F32).astype(BF16)
    weights[5, own_rows, :] = lax.dot_general(
        w_out[...], eye, dims(((0,), (0,))), preferred_element_type=F32
    ).astype(BF16)

    barrier = pltpu.get_barrier_semaphore()
    greeted = 0
    for peer in (
        [{"sp": right}, {"sp": left}]
        + [{"sp": lax.rem(z + BLK, n_sp)}, {"sp": lax.rem(z + n_sp - BLK, n_sp)}]
        + [{"tp": lax.rem(tp + d, n_tp)} for d in range(1, n_tp)]
        + [{"grp": mate}]
    ):
        pl.semaphore_signal(barrier, inc=1, device_id=peer, device_id_type=MESH)
        greeted += 1
    pl.semaphore_wait(barrier, greeted)

    def matrix(slot, par):
        return slot if slot < 2 else slot + 2 * par

    def block(slot, origin, par):
        return weights.at[
            matrix(slot, par), pl.ds(pl.multiple_of(origin * wrows, wrows), wrows)
        ]

    def hop(slot, origin, step, way):
        ref = block(slot, origin, parity)
        return pltpu.make_async_remote_copy(
            src_ref=ref,
            dst_ref=ref,
            send_sem=ring_send.at[way, slot],
            recv_sem=ring_recv.at[way, slot, step],
            device_id={"sp": left if way else right},
            device_id_type=MESH,
        )

    def over(ref, k):
        return pltpu.make_async_remote_copy(
            src_ref=ref,
            dst_ref=ref,
            send_sem=y_send.at[k],
            recv_sem=y_recv.at[k],
            device_id={"grp": mate},
            device_id_type=MESH,
        )

    for slot in range(SLOTS):
        for way in (0, 1):
            hop(slot, z, 1, way).start()

    tok = tokens[...].astype(F32)
    rows = []
    for b in range(seqs):
        part = tok[:, b, :]
        scale = lax.rsqrt(jnp.mean(part * part, axis=-1, keepdims=True) + EPS)
        rows.append(part * scale * gain[...])
    tok_block = pl.ds(pl.multiple_of(here * block_rows, block_rows), block_rows)
    normed[tok_block, :] = jnp.concatenate(rows, axis=0).astype(BF16)

    def token_copy(ref, peer):
        return pltpu.make_async_remote_copy(
            src_ref=ref,
            dst_ref=ref,
            send_sem=tok_send,
            recv_sem=tok_recv,
            device_id={"tp": peer},
            device_id_type=MESH,
        )

    for d in range(1, n_tp):
        token_copy(normed.at[tok_block], lax.rem(tp + d, n_tp)).start()

    def arrive(slot, step, way, forward):
        origin = lax.rem(z + step, n_sp) if way else lax.rem(z + n_sp - step, n_sp)
        hop(slot, origin, step, way).wait_recv()
        if forward is True:
            hop(slot, origin, step + 1, way).start()
        elif forward is not False:
            @pl.when(forward)
            def _():
                hop(slot, origin, step + 1, way).start()
        if slot >= 2:
            over(block(slot, origin, parity), slot - 2).start()

    def ring_step(step, carry):
        for slot in range(SLOTS):
            arrive(slot, step, 0, True)
            arrive(slot, step, 1, step < half - 1)
        return carry

    lax.fori_loop(1, half, ring_step, 0)
    for slot in range(SLOTS):
        arrive(slot, half, 0, False)

    others = block_rows * (n_tp - 1)
    token_copy(normed.at[pl.ds(0, others)], tp).wait_recv()

    def project(m):
        return (
            jnp.dot(normed[...], weights[m], preferred_element_type=F32)
            .astype(BF16)
            .astype(F32)
        )

    def by_sequence(ref, value):
        for t in range(n_tp):
            for b in range(seqs):
                first = spot(t) * block_rows + b * step_pos
                ref[b, t * step_pos : (t + 1) * step_pos, :] = value[
                    first : first + step_pos, :
                ]

    def silu(u):
        return u / (1.0 + jnp.exp(-u))

    by_sequence(vs, project(0))
    by_sequence(kf, gap[0:1, :] / (1.0 + jnp.exp(project(1))))
    for k in range(2):
        theirs = weights.at[2 + k + 2 * (1 - parity), pl.ds(0, wrows * (n_sp - 1))]
        over(theirs, k).wait_recv()
    by_sequence(kb, gap[1:2, :] / (1.0 + jnp.exp(project(2))))

    at_row = lax.broadcasted_iota(jnp.int32, (span, span), 0)
    at_col = lax.broadcasted_iota(jnp.int32, (span, span), 1)
    lower = (at_row >= at_col).astype(F32)
    upper = (at_row <= at_col).astype(F32)
    for b in range(seqs):
        moved = shift[:, b, :]
        fwd_key, bwd_key = kf[b], kb[b]
        fwd_run = jnp.dot(
            lower,
            jnp.log1p(-fwd_key) + moved,
            precision=lax.Precision.HIGHEST,
            preferred_element_type=F32,
        )
        bwd_run = jnp.dot(
            upper,
            jnp.log1p(-bwd_key) + moved,
            precision=lax.Precision.HIGHEST,
            preferred_element_type=F32,
        )
        rf[b] = fwd_run
        rb[b] = bwd_run
        fwd_end, bwd_end = fwd_run[span - 1 : span, :], bwd_run[0:1, :]
        keys = jnp.concatenate(
            [fwd_key * jnp.exp(fwd_end - fwd_run), bwd_key * jnp.exp(bwd_end - bwd_run)],
            axis=1,
        ).astype(BF16)
        states = lax.dot_general(
            vs[b].astype(BF16), keys, dims(((0,), (0,))), preferred_element_type=F32
        )
        for h in range(heads):
            c = b * heads + h
            lanes = slice(h * CH, (h + 1) * CH)
            for d, end in enumerate((fwd_end, bwd_end)):
                local[d, c] = states[lanes, d * width + h * CH : d * width + (h + 1) * CH]
                decay[d, c : c + 1, :] = jnp.exp(end[:, lanes])

    def ends(d):
        place = (n_sp - 1 - z) if d == 1 else z
        return place // BLK, lax.rem(place, BLK), (-1 if d == 1 else 1)

    def scan_copy(src, dst, send, recv, target):
        return pltpu.make_async_remote_copy(
            src_ref=src,
            dst_ref=dst,
            send_sem=send,
            recv_sem=recv,
            device_id={"sp": target},
            device_id_type=MESH,
        )

    def factor(d, way, j):
        return scan_copy(
            decay.at[d], decay_in.at[d, j - 1], d_send.at[d, j - 1], d_recv.at[d, j - 1], z + j * way
        )

    def near(d, way, c):
        return scan_copy(
            sent1.at[d, c], before.at[d, c], p1_send.at[d], p1_recv.at[d, c], z + way
        )

    def far(d, way, c):
        return scan_copy(
            sent2.at[d, c], ahead.at[d, c], p2_send.at[d, 0], p2_recv.at[d, c], z + BLK * way
        )

    def down(d, way, c):
        return scan_copy(
            sent2.at[d, c], ahead.at[d, c], p2_send.at[d, 1], p2_recv.at[d, c], z + way
        )

    def relay(d, way, c):
        return scan_copy(
            ahead.at[d, c], ahead.at[d, c], p2_send.at[d, 1], p2_recv.at[d, c], z + way
        )

    for d in (0, 1):
        jj, rr, way = ends(d)

        @pl.when(jj == 0)
        def _():
            ahead[d] = jnp.zeros(ahead.shape[1:], ahead.dtype)

        @pl.when(rr == 0)
        def _():
            before[d] = jnp.zeros(before.shape[1:], before.dtype)

        for j in range(1, BLK):

            @pl.when(rr + j < BLK)
            def _():
                factor(d, way, j).start()

    def first_pass(d):
        jj, rr, way = ends(d)

        def each(c, carry):

            @pl.when(rr > 0)
            def _():
                near(d, way, c).wait_recv()

            joined = decay[d, pl.ds(c, 1), :] * before[d, c].astype(F32) + local[d, c]

            @pl.when(rr < BLK - 1)
            def _():
                sent1[d, c] = joined.astype(BF16)
                near(d, way, c).start()

            @pl.when(rr == BLK - 1)
            def _():
                total[d, c] = joined

                @pl.when(jj == 0)
                def _():
                    sent2[d, c] = joined.astype(BF16)
                    far(d, way, c).start()
                    down(d, way, c).start()

            return carry

        lax.fori_loop(0, chunks, each, 0)

    early = lax.rem(z, BLK) < BLK // 2

    @pl.when(early)
    def _():
        first_pass(0)
        first_pass(1)

    @pl.when(jnp.logical_not(early))
    def _():
        first_pass(1)
        first_pass(0)

    for d in (0, 1):
        jj, rr, way = ends(d)
        decay_before[d] = jnp.ones(decay_before.shape[1:], F32)
        for j in range(1, BLK):

            @pl.when(rr >= j)
            def _():
                factor(d, way, j).wait_recv()
                decay_before[d] = decay_before[d] * decay_in[d, j - 1]

        decay_sent[d] = decay_before[d] * decay[d]

    def second_pass(d):
        jj, rr, way = ends(d)

        def each(c, carry):
            @pl.when(jj > 0)
            def _():
                far(d, way, c).wait_recv()

            @pl.when((rr == BLK - 1) & (jj > 0) & (jj < n_blocks - 1))
            def _():
                joined = (
                    decay_sent[d, pl.ds(c, 1), :] * ahead[d, c].astype(F32) + total[d, c]
                )
                sent2[d, c] = joined.astype(BF16)
                far(d, way, c).start()
                down(d, way, c).start()

            @pl.when((rr < BLK - 2) & (jj > 0))
            def _():
                relay(d, way, c).start()

            carried[c, :, d * CH : (d + 1) * CH] = (
                decay_before[d, pl.ds(c, 1), :] * ahead[d, c].astype(F32)
                + before[d, c].astype(F32)
            ).astype(BF16)
            return carry

        lax.fori_loop(0, chunks, each, 0)

    def inside():
        by_sequence(qs, silu(project(4)))
        by_sequence(gs, silu(project(3)))
        middle = span // 2 - 1
        for b in range(seqs):
            query, fwd_run, bwd_run = qs[b], rf[b], rb[b]
            fwd_mid, bwd_mid = fwd_run[middle : middle + 1, :], bwd_run[middle : middle + 1, :]
            fwd_q = (query * jnp.exp(fwd_run - fwd_mid)).astype(BF16)
            bwd_q = (query * jnp.exp(bwd_run - bwd_mid)).astype(BF16)
            fwd_k = (kf[b] * jnp.exp(fwd_mid - fwd_run)).astype(BF16)
            bwd_k = (kb[b] * jnp.exp(bwd_mid - bwd_run)).astype(BF16)
            fwd_e = (query * jnp.exp(fwd_run)).astype(BF16)
            bwd_e = (query * jnp.exp(bwd_run)).astype(BF16)
            value = vs[b].astype(BF16)
            for h in range(heads):
                c = b * heads + h
                lanes = slice(h * CH, (h + 1) * CH)
                fwd_s = lax.dot_general(
                    fwd_q[:, lanes], fwd_k[:, lanes], dims(((1,), (1,))), preferred_element_type=F32
                )
                bwd_s = lax.dot_general(
                    bwd_q[:, lanes], bwd_k[:, lanes], dims(((1,), (1,))), preferred_element_type=F32
                )
                scores = jnp.where(at_row >= at_col, fwd_s, 0.0) + jnp.where(
                    at_row <= at_col, bwd_s, 0.0
                )
                inner[c] = jnp.dot(
                    scores.astype(BF16), value[:, lanes], preferred_element_type=F32
                )
                qe[c] = jnp.concatenate([fwd_e[:, lanes], bwd_e[:, lanes]], axis=1)

    low = z < half

    @pl.when(low)
    def _():
        second_pass(0)

    @pl.when(jnp.logical_not(low))
    def _():
        second_pass(1)

    inside()

    @pl.when(low)
    def _():
        second_pass(1)

    @pl.when(jnp.logical_not(low))
    def _():
        second_pass(0)

    for b in range(seqs):
        for h in range(heads):
            c = b * heads + h
            both = inner[c] + lax.dot_general(
                qe[c], carried[c], dims(((1,), (1,))), preferred_element_type=F32
            )
            scale = lax.rsqrt(jnp.mean(both * both, axis=-1, keepdims=True) + EPS)
            gated = both * scale * head_gain[...] * gs[b, :, h * CH : (h + 1) * CH]
            for t in range(n_tp):
                first = spot(t) * block_rows + b * step_pos
                mixed[first : first + step_pos, h * CH : (h + 1) * CH] = gated[
                    t * step_pos : (t + 1) * step_pos, :
                ]

    side = n_x * block_rows

    def partial(which):
        lines = pl.ds(pl.multiple_of(which * side, side), side)
        return lax.dot_general(
            mixed[lines, :].astype(BF16),
            weights[5],
            dims(((1,), (1,))),
            preferred_element_type=F32,
        )

    given[...] = partial(1 - core).astype(BF16)
    pair = pltpu.make_async_remote_copy(
        src_ref=given,
        dst_ref=taken,
        send_sem=pair_send,
        recv_sem=pair_recv,
        device_id={"tp": tp + 1 - 2 * core},
        device_id_type=MESH,
    )
    pair.start()
    mine[...] = partial(core)
    pair.wait_recv()

    def piece(dest, d):
        lines = pl.ds(pl.multiple_of(dest * block_rows, block_rows), block_rows)
        return pltpu.make_async_remote_copy(
            src_ref=summed.at[lines],
            dst_ref=pieces.at[d - 1],
            send_sem=x_send.at[d - 1],
            recv_sem=x_recv.at[d - 1],
            device_id={"tp": dest * 2 + core},
            device_id_type=MESH,
        )

    order = [2, 1, 3] if n_x == 4 else list(range(1, n_x))
    for d in order:
        dest = lax.rem(x + d, n_x)
        lines = pl.ds(pl.multiple_of(dest * block_rows, block_rows), block_rows)
        summed[lines, :] = (mine[lines, :] + taken[lines, :].astype(F32)).astype(BF16)
        piece(dest, d).start()
    own_lines = pl.ds(pl.multiple_of(x * block_rows, block_rows), block_rows)
    result = mine[own_lines, :] + taken[own_lines, :].astype(F32)
    for d in range(1, n_x):
        piece(x, d).wait_recv()
        result = result + pieces[d - 1].astype(F32)
    out[...] = result.astype(BF16)

    for slot in range(SLOTS):
        for way in (0, 1):
            length = wrows * (half - way)
            ref = weights.at[matrix(slot, parity), pl.ds(0, length)]
            pltpu.make_async_remote_copy(
                src_ref=ref,
                dst_ref=ref,
                send_sem=ring_send.at[way, slot],
                recv_sem=ring_recv.at[way, slot, 0],
                device_id={"sp": right},
                device_id_type=MESH,
            ).wait_send()
    for k in range(2):
        over(weights.at[k, pl.ds(0, wrows * (n_sp - 1))], k).wait_send()
    token_copy(normed.at[pl.ds(0, others)], tp).wait_send()
    for d in (0, 1):
        jj, rr, way = ends(d)

        @pl.when(rr < BLK - 1)
        def _():
            scan_copy(sent1.at[d], before.at[d], p1_send.at[d], p1_recv.at[d, 0], z).wait_send()

        for j in range(1, BLK):

            @pl.when(rr + j < BLK)
            def _():
                factor(d, way, j).wait_send()

        leads = (rr == BLK - 1) & (jj < n_blocks - 1)

        @pl.when(leads)
        def _():
            scan_copy(sent2.at[d], ahead.at[d], p2_send.at[d, 0], p2_recv.at[d, 0], z).wait_send()

        @pl.when(leads | ((rr < BLK - 2) & (jj > 0)))
        def _():
            scan_copy(sent2.at[d], ahead.at[d], p2_send.at[d, 1], p2_recv.at[d, 0], z).wait_send()

    pair.wait_send()
    for d in range(1, n_x):
        piece(lax.rem(x + d, n_x), d).wait_send()


def shards(
    n_sp,
    n_tp,
    tokens,
    norm_gain,
    w_query,
    w_value,
    w_fwd_gate,
    w_bwd_gate,
    w_out_gate,
    floor_gap,
    decay_shift,
    head_gain,
    w_out,
):
    step_pos, seqs, model = tokens.shape
    wrows, width = w_query.shape
    span = decay_shift.shape[0]
    chunks = seqs * (width // CH)
    rows = step_pos * seqs
    all_rows = rows * n_tp
    n_x = n_tp // 2
    f32_rows = pltpu.VMEM((seqs, span, width), F32)
    vmem = pl.BlockSpec(memory_space=pltpu.VMEM)
    dma = pltpu.SemaphoreType.DMA
    result = pl.pallas_call(
        functools.partial(kernel, n_sp, n_tp),
        out_shape=jax.ShapeDtypeStruct((rows, model), BF16),
        in_specs=[vmem] * 11,
        out_specs=vmem,
        scratch_shapes=[
            pltpu.VMEM((6, wrows * n_sp, width), BF16),
            pltpu.VMEM((all_rows, model), BF16),
            f32_rows,
            f32_rows,
            f32_rows,
            f32_rows,
            f32_rows,
            f32_rows,
            f32_rows,
            pltpu.VMEM((chunks, span, 2 * CH), BF16),
            pltpu.VMEM((chunks, span, CH), F32),
            pltpu.VMEM((2, chunks, CH, CH), F32),
            pltpu.VMEM((2, chunks, CH), F32),
            pltpu.VMEM((2, chunks, CH, CH), BF16),
            pltpu.VMEM((2, BLK - 1, chunks, CH), F32),
            pltpu.VMEM((2, chunks, CH), F32),
            pltpu.VMEM((2, chunks, CH, CH), BF16),
            pltpu.VMEM((2, chunks, CH), F32),
            pltpu.VMEM((2, chunks, CH, CH), F32),
            pltpu.VMEM((2, chunks, CH, CH), BF16),
            pltpu.VMEM((2, chunks, CH, CH), BF16),
            pltpu.VMEM((chunks, CH, 2 * CH), BF16),
            pltpu.VMEM((all_rows, width), F32),
            pltpu.VMEM((n_x * rows, model), F32),
            pltpu.VMEM((n_x * rows, model), BF16),
            pltpu.VMEM((n_x * rows, model), BF16),
            pltpu.VMEM((n_x * rows, model), BF16),
            pltpu.VMEM((n_x - 1, rows, model), BF16),
            dma((2, SLOTS)),
            dma((2, SLOTS, n_sp // 2 + 1)),
            dma((2,)),
            dma((2,)),
            dma,
            dma,
            dma((2, BLK - 1)),
            dma((2, BLK - 1)),
            dma((2,)),
            dma((2, chunks)),
            dma((2, 2)),
            dma((2, chunks)),
            dma,
            dma,
            dma((n_x - 1,)),
            dma((n_x - 1,)),
        ],
        compiler_params=pltpu.CompilerParams(
            collective_id=0, has_side_effects=True, vmem_limit_bytes=60 * 1024 * 1024
        ),
        name="mixer",
    )(
        tokens,
        norm_gain.reshape(1, -1),
        w_query,
        w_value,
        w_fwd_gate,
        w_bwd_gate,
        w_out_gate,
        w_out,
        floor_gap,
        decay_shift,
        head_gain.reshape(1, -1),
    )
    return result.reshape(seqs, step_pos, model).transpose(1, 0, 2)


def solution(mesh):
    in_specs = (
        P(("sp", "tp"), "grp", None),
        P(),
        P("sp", "tp"),
        P("sp", "tp"),
        P("sp", "tp"),
        P("sp", "tp"),
        P("sp", "tp"),
        P(None, "tp"),
        P("sp", "grp", "tp"),
        P(),
        P("tp", "sp"),
    )
    return jax.shard_map(
        functools.partial(shards, mesh.shape["sp"], mesh.shape["tp"]),
        mesh=mesh,
        in_specs=in_specs,
        out_specs=P(("sp", "tp"), "grp", None),
        check_vma=False,
    )
```

```python
import functools

import jax
import jax.numpy as jnp
from jax import lax
from jax.experimental import pallas as pl
from jax.experimental.pallas import tpu as pltpu
from jax.sharding import PartitionSpec as P

MESH = pl.DeviceIdType.MESH
F32 = jnp.float32
BF16 = jnp.bfloat16
CH = 128
BLK = 4
RING = 3
CARRIER = 1
PARTS = 2
STRIPS = 2
LAG = 7
EPS = 1e-06


def dims(contract):
    return (contract, ((), ()))


def kernel(
    n_sp,
    n_tp,
    tokens,
    gain,
    w_query,
    w_value,
    w_fwd,
    w_bwd,
    w_gate,
    w_out,
    gap,
    shift,
    head_gain,
    out,
    weights,
    others,
    normed,
    gap_there,
    shift_there,
    vs_there,
    kf_there,
    kb_there,
    rf_there,
    rb_there,
    qs,
    vs,
    kf,
    kb,
    rf,
    rb,
    gs,
    qe,
    inner,
    local,
    decay,
    before,
    decay_in,
    decay_before,
    sent1,
    decay_sent,
    total,
    ahead,
    sent2,
    carried,
    mixed,
    mine,
    given,
    taken,
    summed,
    pieces,
    ring_send,
    ring_recv,
    first_send,
    push_send,
    push_recv,
    y_send,
    y_recv,
    tok_send,
    tok_recv,
    lend_send,
    lend_recv,
    own_send,
    own_recv,
    hand_send,
    hand_recv,
    back_send,
    back_recv,
    d_send,
    d_recv,
    p1_send,
    p1_recv,
    p2_send,
    p2_recv,
    pair_send,
    pair_recv,
    x_send,
    x_recv,
):
    z = lax.axis_index("sp")
    tp = lax.axis_index("tp")
    grp = lax.axis_index("grp")
    parity = lax.rem(grp, 2)
    mate = grp + 1 - 2 * parity
    right, left = lax.rem(z + 1, n_sp), lax.rem(z + n_sp - 1, n_sp)
    n_x = n_tp // 2
    core, x = lax.rem(tp, 2), tp // 2
    partner = tp + 1 - 2 * core
    carrier = core == CARRIER
    wrows, width = w_query.shape
    step_pos, seqs, model = tokens.shape
    span = shift.shape[0]
    heads = width // CH
    chunks = seqs * heads
    n_blocks = n_sp // BLK
    block_rows = step_pos * seqs
    half = n_sp // 2

    def spot(t):
        return (t % 2) * n_x + t // 2

    here = spot(tp)

    own_rows = pl.ds(pl.multiple_of(z * wrows, wrows), wrows)
    for m, ref in enumerate((w_value, w_fwd, w_bwd, w_out, w_gate, w_query)):
        weights[m, own_rows, :] = ref[...]

    barrier = pltpu.get_barrier_semaphore()
    greeted = 0
    for peer in (
        [{"sp": a, "tp": b} for a in (right, left) for b in (tp, partner)]
        + [{"tp": lax.rem(tp + d, n_tp)} for d in range(1, n_tp)]
        + [{"grp": mate, "tp": b} for b in (tp, partner)]
    ):
        pl.semaphore_signal(barrier, inc=1, device_id=peer, device_id_type=MESH)
        greeted += 1
    pl.semaphore_wait(barrier, greeted)

    share = wrows // PARTS

    def block(ref, m, origin, p):
        return ref.at[m, pl.ds(pl.multiple_of(origin * wrows + p * share, share), share)]

    def which(i):
        return i * (1 + parity)

    def held(base, i, owner, origin, p):
        if owner:
            return block(others, which(i), origin, p)
        return block(weights, base + which(i), origin, p)

    def hop(base, i, owner, origin, step, way, p):
        ref = held(base, i, owner, origin, p)
        return pltpu.make_async_remote_copy(
            src_ref=ref,
            dst_ref=ref,
            send_sem=ring_send.at[way, i, owner],
            recv_sem=ring_recv.at[way, i, owner, step, p],
            device_id={"sp": left if way else right},
            device_id_type=MESH,
        )

    def enter(base, i, way, p):
        return pltpu.make_async_remote_copy(
            src_ref=block(weights, base + which(i), z, p),
            dst_ref=block(others, which(i), z, p),
            send_sem=first_send.at[way, i, p],
            recv_sem=ring_recv.at[way, i, 1, 1, p],
            device_id={"sp": left if way else right, "tp": partner},
            device_id_type=MESH,
        )

    def push(src, dst, i):
        return pltpu.make_async_remote_copy(
            src_ref=src,
            dst_ref=dst,
            send_sem=push_send.at[i],
            recv_sem=push_recv.at[i],
            device_id={"tp": partner},
            device_id_type=MESH,
        )

    def over(src, dst, base, owner):
        return pltpu.make_async_remote_copy(
            src_ref=src,
            dst_ref=dst,
            send_sem=y_send.at[owner],
            recv_sem=y_recv.at[2 if base else owner],
            device_id={"grp": mate, "tp": partner if base and owner else tp},
            device_id_type=MESH,
        )

    def open_ring(base):
        for i in range(2):
            for p in range(PARTS):
                for way in (0, 1):
                    hop(base, i, 0, z, 1, way, p).start()

    def join_ring(base):
        for i in range(2):
            for p in range(PARTS):
                for way in (0, 1):
                    enter(base, i, way, p).start()

    def arrive(base, i, owner, step, way, p, forward):
        origin = lax.rem(z + step, n_sp) if way else lax.rem(z + n_sp - step, n_sp)
        hop(base, i, owner, origin, step, way, p).wait_recv()
        if forward is True:
            hop(base, i, owner, origin, step + 1, way, p).start()
        elif forward is not False:

            @pl.when(forward)
            def _():
                hop(base, i, owner, origin, step + 1, way, p).start()

        mine = held(base, i, owner, origin, p)
        home = block(weights, base + which(i), origin, p)
        if i:
            over(mine, home if base else mine, base, owner).start()
        if base and owner:
            push(mine, home, i).start()

    streams = [(i, owner, p) for i in (1, 0) for owner in (0, 1) for p in range(PARTS)]

    def carry_ring(base):
        def ring_step(step, carry):
            for i, owner, p in streams:
                arrive(base, i, owner, step, 0, p, True)
                arrive(base, i, owner, step, 1, p, step < half - 1)
            return carry

        lax.fori_loop(1, half, ring_step, 0)
        for i, owner, p in streams:
            arrive(base, i, owner, half, 0, p, False)

    def pushed():
        for i in range(2):
            ref = weights.at[RING + which(i), pl.ds(0, wrows * (n_sp - 1))]
            push(ref, ref, i).wait_recv()

    def came_over(base, owner):
        ref = weights.at[base + 2 - parity, pl.ds(0, wrows * (n_sp - 1))]
        over(ref, ref, base, owner).wait_recv()

    def pair_copy(src, dst, send, recv):
        return pltpu.make_async_remote_copy(
            src_ref=src,
            dst_ref=dst,
            send_sem=send,
            recv_sem=recv,
            device_id={"tp": partner},
            device_id_type=MESH,
        )

    def lend(k):
        src, dst = ((gap, gap_there), (shift, shift_there))[k]
        return pair_copy(src, dst, lend_send.at[k], lend_recv.at[k])

    def own_block(m):
        lines = pl.ds(pl.multiple_of(z * wrows, wrows), wrows)
        return pair_copy(
            weights.at[m, lines], others.at[m, lines], own_send.at[m], own_recv.at[m]
        )

    def hand(k):
        src = (vs_there, kf_there, kb_there, rf_there, rb_there)[k]
        dst = (vs, kf, kb, rf, rb)[k]
        return pair_copy(src, dst, hand_send.at[k], hand_recv.at[k])

    @pl.when(carrier)
    def _():
        open_ring(0)
        join_ring(RING)

    @pl.when(jnp.logical_not(carrier))
    def _():
        join_ring(0)
        open_ring(RING)
        for k in range(2):
            lend(k).start()
        for m in range(RING):
            own_block(m).start()

    tok = tokens[...].astype(F32)
    rows = []
    for b in range(seqs):
        part = tok[:, b, :]
        scale = lax.rsqrt(jnp.mean(part * part, axis=-1, keepdims=True) + EPS)
        rows.append(part * scale * gain[...])
    tok_block = pl.ds(pl.multiple_of(here * block_rows, block_rows), block_rows)
    normed[tok_block, :] = jnp.concatenate(rows, axis=0).astype(BF16)

    def token_copy(ref, peer):
        return pltpu.make_async_remote_copy(
            src_ref=ref,
            dst_ref=ref,
            send_sem=tok_send,
            recv_sem=tok_recv,
            device_id={"tp": peer},
            device_id_type=MESH,
        )

    for d in range(1, n_tp):
        token_copy(normed.at[tok_block], lax.rem(tp + d, n_tp)).start()

    @pl.when(carrier)
    def _():
        carry_ring(0)

    rest = normed.at[pl.ds(0, block_rows * (n_tp - 1))]

    def project(matrix):
        return (
            jnp.dot(normed[...], matrix, preferred_element_type=F32).astype(BF16).astype(F32)
        )

    def by_sequence(ref, value):
        for t in range(n_tp):
            for b in range(seqs):
                first = spot(t) * block_rows + b * step_pos
                ref[b, t * step_pos : (t + 1) * step_pos, :] = value[
                    first : first + step_pos, :
                ]

    def silu(u):
        return u / (1.0 + jnp.exp(-u))

    at_row = lax.broadcasted_iota(jnp.int32, (span, span), 0)
    at_col = lax.broadcasted_iota(jnp.int32, (span, span), 1)
    lower = (at_row >= at_col).astype(F32)
    upper = (at_row <= at_col).astype(F32)
    def prepare(matrices, gap_ref, shift_ref, vs_ref, kf_ref, kb_ref, rf_ref, rb_ref, base):
        by_sequence(vs_ref, project(matrices[0]))
        by_sequence(kf_ref, gap_ref[0:1, :] / (1.0 + jnp.exp(project(matrices[1]))))
        by_sequence(kb_ref, gap_ref[1:2, :] / (1.0 + jnp.exp(project(matrices[2]))))
        for b in range(seqs):
            moved = shift_ref[:, b, :]
            fwd_key, bwd_key = kf_ref[b], kb_ref[b]
            fwd_run = jnp.dot(
                lower,
                jnp.log1p(-fwd_key) + moved,
                precision=lax.Precision.HIGHEST,
                preferred_element_type=F32,
            )
            bwd_run = jnp.dot(
                upper,
                jnp.log1p(-bwd_key) + moved,
                precision=lax.Precision.HIGHEST,
                preferred_element_type=F32,
            )
            rf_ref[b] = fwd_run
            rb_ref[b] = bwd_run
            fwd_end, bwd_end = fwd_run[span - 1 : span, :], bwd_run[0:1, :]
            keys = jnp.concatenate(
                [fwd_key * jnp.exp(fwd_end - fwd_run), bwd_key * jnp.exp(bwd_end - bwd_run)],
                axis=1,
            ).astype(BF16)
            states = lax.dot_general(
                vs_ref[b].astype(BF16), keys, dims(((0,), (0,))), preferred_element_type=F32
            )
            for h in range(heads):
                c = b * heads + h
                lanes = slice(h * CH, (h + 1) * CH)
                for d, end in enumerate((fwd_end, bwd_end)):
                    local[d, base + c] = states[
                        lanes, d * width + h * CH : d * width + (h + 1) * CH
                    ].astype(BF16)
                    decay[d, base + c : base + c + 1, :] = jnp.exp(end[:, lanes])

    low_chunks = pl.ds(0, chunks)

    def give_back(d, c):
        return pair_copy(carried.at[d, c], carried.at[d, c - chunks], back_send.at[d], back_recv.at[d])

    def given_back(d):
        ref = carried.at[d, low_chunks]
        return pair_copy(ref, ref, back_send.at[d], back_recv.at[d])

    def ends(d):
        place = (n_sp - 1 - z) if d == 1 else z
        return place // BLK, lax.rem(place, BLK), (-1 if d == 1 else 1)

    def scan_copy(src, dst, send, recv, target):
        return pltpu.make_async_remote_copy(
            src_ref=src,
            dst_ref=dst,
            send_sem=send,
            recv_sem=recv,
            device_id={"sp": target},
            device_id_type=MESH,
        )

    def factor(d, way, j):
        return scan_copy(
            decay.at[d], decay_in.at[d, j - 1], d_send.at[d, j - 1], d_recv.at[d, j - 1], z + j * way
        )

    def near(d, way, c):
        return scan_copy(
            sent1.at[d, c], before.at[d, c], p1_send.at[d], p1_recv.at[d, c], z + way
        )

    def far(d, way, c):
        return scan_copy(
            sent2.at[d, c], ahead.at[d, c], p2_send.at[d, 0], p2_recv.at[d, c], z + BLK * way
        )

    def down(d, way, c):
        return scan_copy(
            sent2.at[d, c], ahead.at[d, c], p2_send.at[d, 1], p2_recv.at[d, c], z + way
        )

    def relay(d, way, c):
        return scan_copy(
            ahead.at[d, c], ahead.at[d, c], p2_send.at[d, 1], p2_recv.at[d, c], z + way
        )

    def clear():
        for d in (0, 1):
            jj, rr, way = ends(d)

            @pl.when(jj == 0)
            def _():
                ahead[d] = jnp.zeros(ahead.shape[1:], ahead.dtype)

            @pl.when(rr == 0)
            def _():
                before[d] = jnp.zeros(before.shape[1:], before.dtype)

    def exchange():
        for d in (0, 1):
            jj, rr, way = ends(d)
            for j in range(1, BLK):

                @pl.when(rr + j < BLK)
                def _():
                    factor(d, way, j).start()

    edge = (lax.rem(z, BLK) == 0) | (lax.rem(z, BLK) == BLK - 1)

    def first_step(d, c):
        jj, rr, way = ends(d)

        @pl.when(rr > 0)
        def _():
            near(d, way, c).wait_recv()

        joined = decay[d, pl.ds(c, 1), :] * before[d, c].astype(F32) + local[d, c].astype(F32)

        @pl.when(rr < BLK - 1)
        def _():
            sent1[d, c] = joined.astype(BF16)
            near(d, way, c).start()

        @pl.when(rr == BLK - 1)
        def _():
            total[d, c] = joined

            @pl.when(jj == 0)
            def _():
                sent2[d, c] = joined.astype(BF16)
                far(d, way, c).start()
                down(d, way, c).start()

    def head_start(d):
        def each(c, carry):
            first_step(d, c)
            return carry

        lax.fori_loop(0, chunks, each, 0)

    def first_pass(d, begin, lag):
        def each(turn, carry):
            @pl.when(turn < 2 * chunks)
            def _():
                first_step(d, turn)

            @pl.when(turn >= lag)
            def _():
                first_step(1 - d, turn - lag)

            return carry

        lax.fori_loop(begin, 2 * chunks + lag, each, 0)

    def factors():
        for d in (0, 1):
            jj, rr, way = ends(d)
            decay_before[d] = jnp.ones(decay_before.shape[1:], F32)
            for j in range(1, BLK):

                @pl.when(rr >= j)
                def _():
                    factor(d, way, j).wait_recv()
                    decay_before[d] = decay_before[d] * decay_in[d, j - 1]

            decay_sent[d] = decay_before[d] * decay[d]

    def second_pass(d):
        jj, rr, way = ends(d)

        def each(c, carry):
            @pl.when(jj > 0)
            def _():
                far(d, way, c).wait_recv()

            @pl.when((rr == BLK - 1) & (jj > 0) & (jj < n_blocks - 1))
            def _():
                joined = (
                    decay_sent[d, pl.ds(c, 1), :] * ahead[d, c].astype(F32) + total[d, c]
                )
                sent2[d, c] = joined.astype(BF16)
                far(d, way, c).start()
                down(d, way, c).start()

            @pl.when((rr < BLK - 2) & (jj > 0))
            def _():
                relay(d, way, c).start()

            carried[d, c] = (
                decay_before[d, pl.ds(c, 1), :] * ahead[d, c].astype(F32)
                + before[d, c].astype(F32)
            ).astype(BF16)

            @pl.when(c >= chunks)
            def _():
                give_back(d, c).start()

            return carry

        lax.fori_loop(0, 2 * chunks, each, 0)

    def inside():
        by_sequence(qs, silu(project(weights[5])))
        by_sequence(gs, silu(project(weights[4])))
        middle = span // 2 - 1
        for b in range(seqs):
            query, fwd_run, bwd_run = qs[b], rf[b], rb[b]
            fwd_mid, bwd_mid = fwd_run[middle : middle + 1, :], bwd_run[middle : middle + 1, :]
            fwd_q = (query * jnp.exp(fwd_run - fwd_mid)).astype(BF16)
            bwd_q = (query * jnp.exp(bwd_run - bwd_mid)).astype(BF16)
            fwd_k = (kf[b] * jnp.exp(fwd_mid - fwd_run)).astype(BF16)
            bwd_k = (kb[b] * jnp.exp(bwd_mid - bwd_run)).astype(BF16)
            fwd_e = (query * jnp.exp(fwd_run)).astype(BF16)
            bwd_e = (query * jnp.exp(bwd_run)).astype(BF16)
            value = vs[b].astype(BF16)
            for h in range(heads):
                c = b * heads + h
                lanes = slice(h * CH, (h + 1) * CH)
                fwd_s = lax.dot_general(
                    fwd_q[:, lanes], fwd_k[:, lanes], dims(((1,), (1,))), preferred_element_type=F32
                )
                bwd_s = lax.dot_general(
                    bwd_q[:, lanes], bwd_k[:, lanes], dims(((1,), (1,))), preferred_element_type=F32
                )
                scores = jnp.where(at_row >= at_col, fwd_s, 0.0) + jnp.where(
                    at_row <= at_col, bwd_s, 0.0
                )
                inner[c] = jnp.dot(
                    scores.astype(BF16), value[:, lanes], preferred_element_type=F32
                )
                qe[c] = jnp.concatenate([fwd_e[:, lanes], bwd_e[:, lanes]], axis=1)

    early = lax.rem(z, BLK) < BLK // 2
    low = z < half

    @pl.when(carrier)
    def _():
        for owner in (0, 1):
            came_over(0, owner)
        clear()
        token_copy(rest, tp).wait_recv()
        prepare([weights[m] for m in range(RING)], gap, shift, vs, kf, kb, rf, rb, 0)

        @pl.when(early & edge)
        def _():
            head_start(0)

        @pl.when(jnp.logical_not(early) & edge)
        def _():
            head_start(1)

        for k in range(2):
            lend(k).wait_recv()
        for m in range(RING):
            own_block(m).wait_recv()
        prepare(
            [others[m] for m in range(RING)],
            gap_there,
            shift_there,
            vs_there,
            kf_there,
            kb_there,
            rf_there,
            rb_there,
            chunks,
        )
        exchange()
        for k in range(5):
            hand(k).start()
        begin = jnp.where(edge, chunks, 0)
        lag = jnp.where(edge, 2 * chunks, LAG)

        @pl.when(early)
        def _():
            first_pass(0, begin, lag)

        @pl.when(jnp.logical_not(early))
        def _():
            first_pass(1, begin, lag)

        factors()

        @pl.when(low)
        def _():
            second_pass(0)

        @pl.when(jnp.logical_not(low))
        def _():
            second_pass(1)

        pushed()

    @pl.when(jnp.logical_not(carrier))
    def _():
        carry_ring(RING)
        token_copy(rest, tp).wait_recv()
        for k in range(5):
            hand(k).wait_recv()

    came_over(RING, 1)
    inside()

    @pl.when(carrier)
    def _():
        @pl.when(low)
        def _():
            second_pass(1)

        @pl.when(jnp.logical_not(low))
        def _():
            second_pass(0)

    @pl.when(jnp.logical_not(carrier))
    def _():
        for d in (0, 1):
            given_back(d).wait_recv()

    for b in range(seqs):
        for h in range(heads):
            c = b * heads + h
            both = inner[c] + lax.dot_general(
                qe[c],
                jnp.concatenate([carried[0, c], carried[1, c]], axis=1),
                dims(((1,), (1,))),
                preferred_element_type=F32,
            )
            scale = lax.rsqrt(jnp.mean(both * both, axis=-1, keepdims=True) + EPS)
            gated = both * scale * head_gain[...] * gs[b, :, h * CH : (h + 1) * CH]
            for t in range(n_tp):
                first = spot(t) * block_rows + b * step_pos
                mixed[first : first + step_pos, h * CH : (h + 1) * CH] = gated[
                    t * step_pos : (t + 1) * step_pos, :
                ]

    side = n_x * block_rows

    def partial(core_index, k):
        lines = pl.ds(pl.multiple_of(core_index * side, side), side)
        return lax.dot_general(
            mixed[lines, :].astype(BF16),
            weights[3, k * (model // STRIPS) : (k + 1) * (model // STRIPS), :],
            dims(((1,), (1,))),
            preferred_element_type=F32,
        )

    strip = model // STRIPS

    def exchange_pair(k):
        columns = pl.ds(k * strip, strip)
        return pair_copy(
            given.at[:, columns], taken.at[:, columns], pair_send.at[k], pair_recv.at[k]
        )

    def piece(dest, d, k):
        lines = pl.ds(pl.multiple_of(dest * block_rows, block_rows), block_rows)
        columns = pl.ds(k * strip, strip)
        return pltpu.make_async_remote_copy(
            src_ref=summed.at[lines, columns],
            dst_ref=pieces.at[d - 1, :, columns],
            send_sem=x_send.at[d - 1, k],
            recv_sem=x_recv.at[d - 1, k],
            device_id={"tp": dest * 2 + core},
            device_id_type=MESH,
        )

    for k in range(STRIPS):
        given[:, k * strip : (k + 1) * strip] = partial(1 - core, k).astype(BF16)
        exchange_pair(k).start()
    for k in range(STRIPS):
        mine[:, k * strip : (k + 1) * strip] = partial(core, k)
    order = [2, 1, 3] if n_x == 4 else list(range(1, n_x))
    for k in range(STRIPS):
        exchange_pair(k).wait_recv()
        columns = slice(k * strip, (k + 1) * strip)
        for d in order:
            dest = lax.rem(x + d, n_x)
            lines = pl.ds(pl.multiple_of(dest * block_rows, block_rows), block_rows)
            summed[lines, columns] = (
                mine[lines, columns] + taken[lines, columns].astype(F32)
            ).astype(BF16)
            piece(dest, d, k).start()
    own_lines = pl.ds(pl.multiple_of(x * block_rows, block_rows), block_rows)
    for k in range(STRIPS):
        columns = slice(k * strip, (k + 1) * strip)
        result = mine[own_lines, columns] + taken[own_lines, columns].astype(F32)
        for d in order:
            piece(x, d, k).wait_recv()
            result = result + pieces[d - 1, :, columns].astype(F32)
        out[:, columns] = result.astype(BF16)

    def ring_left(ref, count, way, i, owner):
        lines = ref.at[0, pl.ds(0, wrows * count)]
        pltpu.make_async_remote_copy(
            src_ref=lines,
            dst_ref=lines,
            send_sem=ring_send.at[way, i, owner],
            recv_sem=ring_recv.at[way, i, owner, 0, 0],
            device_id={"sp": right},
            device_id_type=MESH,
        ).wait_send()

    for i in range(2):
        for way in (0, 1):
            ring_left(weights, half - way, way, i, 0)
            ring_left(weights, half - 1 - way, way, i, 1)
            for p in range(PARTS):
                enter(0, i, way, p).wait_send()
        lines = weights.at[0, pl.ds(0, wrows * (n_sp - 1))]
        over(lines, lines, 0, i).wait_send()
    token_copy(rest, tp).wait_send()
    @pl.when(carrier)
    def _():
        for d in (0, 1):
            jj, rr, way = ends(d)

            @pl.when(rr < BLK - 1)
            def _():
                scan_copy(sent1.at[d], before.at[d], p1_send.at[d], p1_recv.at[d, 0], z).wait_send()

            for j in range(1, BLK):

                @pl.when(rr + j < BLK)
                def _():
                    factor(d, way, j).wait_send()

            leads = (rr == BLK - 1) & (jj < n_blocks - 1)

            @pl.when(leads)
            def _():
                scan_copy(sent2.at[d], ahead.at[d], p2_send.at[d, 0], p2_recv.at[d, 0], z).wait_send()

            @pl.when(leads | ((rr < BLK - 2) & (jj > 0)))
            def _():
                scan_copy(sent2.at[d], ahead.at[d], p2_send.at[d, 1], p2_recv.at[d, 0], z).wait_send()
            given_back(d).wait_send()
        for k in range(5):
            hand(k).wait_send()

    @pl.when(jnp.logical_not(carrier))
    def _():
        for m in range(RING):
            own_block(m).wait_send()
        for k in range(2):
            lend(k).wait_send()
            lines = weights.at[0, pl.ds(0, wrows * (n_sp - 1))]
            push(lines, lines, k).wait_send()

    for k in range(STRIPS):
        exchange_pair(k).wait_send()
        for d in order:
            piece(lax.rem(x + d, n_x), d, k).wait_send()


def shards(
    n_sp,
    n_tp,
    tokens,
    norm_gain,
    w_query,
    w_value,
    w_fwd_gate,
    w_bwd_gate,
    w_out_gate,
    floor_gap,
    decay_shift,
    head_gain,
    w_out,
):
    step_pos, seqs, model = tokens.shape
    wrows, width = w_query.shape
    span = decay_shift.shape[0]
    chunks = seqs * (width // CH)
    both = 2 * chunks
    rows = step_pos * seqs
    all_rows = rows * n_tp
    n_x = n_tp // 2
    f32_rows = pltpu.VMEM((seqs, span, width), F32)
    vmem = pl.BlockSpec(memory_space=pltpu.VMEM)
    dma = pltpu.SemaphoreType.DMA
    result = pl.pallas_call(
        functools.partial(kernel, n_sp, n_tp),
        out_shape=jax.ShapeDtypeStruct((rows, model), BF16),
        in_specs=[vmem] * 11,
        out_specs=vmem,
        scratch_shapes=[
            pltpu.VMEM((6, wrows * n_sp, width), BF16),
            pltpu.VMEM((RING, wrows * n_sp, width), BF16),
            pltpu.VMEM((all_rows, model), BF16),
            pltpu.VMEM((2, width), F32),
            pltpu.VMEM((span, seqs, width), F32),
            f32_rows,
            f32_rows,
            f32_rows,
            f32_rows,
            f32_rows,
            f32_rows,
            f32_rows,
            f32_rows,
            f32_rows,
            f32_rows,
            f32_rows,
            f32_rows,
            pltpu.VMEM((chunks, span, 2 * CH), BF16),
            pltpu.VMEM((chunks, span, CH), F32),
            pltpu.VMEM((2, both, CH, CH), BF16),
            pltpu.VMEM((2, both, CH), F32),
            pltpu.VMEM((2, both, CH, CH), BF16),
            pltpu.VMEM((2, BLK - 1, both, CH), F32),
            pltpu.VMEM((2, both, CH), F32),
            pltpu.VMEM((2, both, CH, CH), BF16),
            pltpu.VMEM((2, both, CH), F32),
            pltpu.VMEM((2, both, CH, CH), F32),
            pltpu.VMEM((2, both, CH, CH), BF16),
            pltpu.VMEM((2, both, CH, CH), BF16),
            pltpu.VMEM((2, both, CH, CH), BF16),
            pltpu.VMEM((all_rows, width), F32),
            pltpu.VMEM((n_x * rows, model), F32),
            pltpu.VMEM((n_x * rows, model), BF16),
            pltpu.VMEM((n_x * rows, model), BF16),
            pltpu.VMEM((n_x * rows, model), BF16),
            pltpu.VMEM((n_x - 1, rows, model), BF16),
            dma((2, 2, 2)),
            dma((2, 2, 2, n_sp // 2 + 1, PARTS)),
            dma((2, 2, PARTS)),
            dma((2,)),
            dma((2,)),
            dma((2,)),
            dma((3,)),
            dma,
            dma,
            dma((2,)),
            dma((2,)),
            dma((RING,)),
            dma((RING,)),
            dma((5,)),
            dma((5,)),
            dma((2,)),
            dma((2,)),
            dma((2, BLK - 1)),
            dma((2, BLK - 1)),
            dma((2,)),
            dma((2, both)),
            dma((2, 2)),
            dma((2, both)),
            dma((STRIPS,)),
            dma((STRIPS,)),
            dma((n_x - 1, STRIPS)),
            dma((n_x - 1, STRIPS)),
        ],
        compiler_params=pltpu.CompilerParams(
            collective_id=0, has_side_effects=True, vmem_limit_bytes=60 * 1024 * 1024
        ),
        name="mixer",
    )(
        tokens,
        norm_gain.reshape(1, -1),
        w_query,
        w_value,
        w_fwd_gate,
        w_bwd_gate,
        w_out_gate,
        w_out.T,
        floor_gap,
        decay_shift,
        head_gain.reshape(1, -1),
    )
    return result.reshape(seqs, step_pos, model).transpose(1, 0, 2)


def solution(mesh):
    in_specs = (
        P(("sp", "tp"), "grp", None),
        P(),
        P("sp", "tp"),
        P("sp", "tp"),
        P("sp", "tp"),
        P("sp", "tp"),
        P("sp", "tp"),
        P(None, "tp"),
        P("sp", "grp", "tp"),
        P(),
        P("tp", "sp"),
    )
    return jax.shard_map(
        functools.partial(shards, mesh.shape["sp"], mesh.shape["tp"]),
        mesh=mesh,
        in_specs=in_specs,
        out_specs=P(("sp", "tp"), "grp", None),
        check_vma=False,
    )
```

```python
import functools

import jax
import jax.numpy as jnp
from jax import lax
from jax.experimental import pallas as pl
from jax.experimental.pallas import tpu as pltpu
from jax.sharding import PartitionSpec as P

MESH = pl.DeviceIdType.MESH
F32 = jnp.float32
BF16 = jnp.bfloat16
CH = 128
BLK = 4
RING = 3
CARRIER = 1
PARTS = 2
STRIPS = 2
LAG = 7
EPS = 1e-06


def dims(contract):
    return (contract, ((), ()))


def kernel(
    n_sp,
    n_tp,
    tokens_in,
    gain_in,
    w_query,
    w_value,
    w_fwd,
    w_bwd,
    w_gate,
    w_out,
    gap_in,
    shift_in,
    head_gain_in,
    out,
    tokens,
    gain,
    gap,
    shift,
    head_gain,
    weights,
    others,
    normed,
    gap_there,
    shift_there,
    vs_there,
    kf_there,
    kb_there,
    rf_there,
    rb_there,
    qs,
    vs,
    kf,
    kb,
    rf,
    rb,
    gs,
    qe,
    inner,
    local,
    decay,
    before,
    decay_in,
    decay_before,
    sent1,
    decay_sent,
    total,
    ahead,
    sent2,
    carried,
    mixed,
    mine,
    given,
    taken,
    summed,
    pieces,
    ring_send,
    ring_recv,
    first_send,
    push_send,
    push_recv,
    y_send,
    y_recv,
    tok_send,
    tok_recv,
    lend_send,
    lend_recv,
    own_send,
    own_recv,
    hand_send,
    hand_recv,
    back_send,
    back_recv,
    d_send,
    d_recv,
    p1_send,
    p1_recv,
    p2_send,
    p2_recv,
    pair_send,
    pair_recv,
    x_send,
    x_recv,
    load_sem,
):
    z = lax.axis_index("sp")
    tp = lax.axis_index("tp")
    grp = lax.axis_index("grp")
    parity = lax.rem(grp, 2)
    mate = grp + 1 - 2 * parity
    right, left = lax.rem(z + 1, n_sp), lax.rem(z + n_sp - 1, n_sp)
    n_x = n_tp // 2
    core, x = lax.rem(tp, 2), tp // 2
    partner = tp + 1 - 2 * core
    carrier = core == CARRIER
    wrows, width = w_query.shape
    step_pos, seqs, model = tokens.shape
    span = shift.shape[0]
    heads = width // CH
    chunks = seqs * heads
    n_blocks = n_sp // BLK
    block_rows = step_pos * seqs
    half = n_sp // 2

    def spot(t):
        return (t % 2) * n_x + t // 2

    here = spot(tp)

    own_rows = pl.ds(pl.multiple_of(z * wrows, wrows), wrows)
    loads = [
        (ref, weights.at[m, own_rows])
        for m, ref in enumerate((w_value, w_fwd, w_bwd, w_out, w_gate, w_query))
    ] + [
        (tokens_in, tokens),
        (gain_in, gain),
        (gap_in, gap),
        (shift_in, shift),
        (head_gain_in, head_gain),
    ]
    loads = [
        pltpu.make_async_copy(src, dst, load_sem.at[k]) for k, (src, dst) in enumerate(loads)
    ]

    barrier = pltpu.get_barrier_semaphore()
    greeted = 0
    for peer in (
        [{"sp": a, "tp": b} for a in (right, left) for b in (tp, partner)]
        + [{"tp": lax.rem(tp + d, n_tp)} for d in range(1, n_tp)]
        + [{"grp": mate, "tp": b} for b in (tp, partner)]
    ):
        pl.semaphore_signal(barrier, inc=1, device_id=peer, device_id_type=MESH)
        greeted += 1
    for load in loads:
        load.start()
    pl.semaphore_wait(barrier, greeted)
    for load in loads[:6]:
        load.wait()

    share = wrows // PARTS

    def block(ref, m, origin, p):
        return ref.at[m, pl.ds(pl.multiple_of(origin * wrows + p * share, share), share)]

    def which(i):
        return i * (1 + parity)

    def held(base, i, owner, origin, p):
        if owner:
            return block(others, which(i), origin, p)
        return block(weights, base + which(i), origin, p)

    def hop(base, i, owner, origin, step, way, p):
        ref = held(base, i, owner, origin, p)
        return pltpu.make_async_remote_copy(
            src_ref=ref,
            dst_ref=ref,
            send_sem=ring_send.at[way, i, owner],
            recv_sem=ring_recv.at[way, i, owner, step, p],
            device_id={"sp": left if way else right},
            device_id_type=MESH,
        )

    def enter(base, i, way, p):
        return pltpu.make_async_remote_copy(
            src_ref=block(weights, base + which(i), z, p),
            dst_ref=block(others, which(i), z, p),
            send_sem=first_send.at[way, i, p],
            recv_sem=ring_recv.at[way, i, 1, 1, p],
            device_id={"sp": left if way else right, "tp": partner},
            device_id_type=MESH,
        )

    def push(src, dst, i):
        return pltpu.make_async_remote_copy(
            src_ref=src,
            dst_ref=dst,
            send_sem=push_send.at[i],
            recv_sem=push_recv.at[i],
            device_id={"tp": partner},
            device_id_type=MESH,
        )

    def over(src, dst, base, owner):
        return pltpu.make_async_remote_copy(
            src_ref=src,
            dst_ref=dst,
            send_sem=y_send.at[owner],
            recv_sem=y_recv.at[2 if base else owner],
            device_id={"grp": mate, "tp": partner if base and owner else tp},
            device_id_type=MESH,
        )

    def open_ring(base):
        for i in range(2):
            for p in range(PARTS):
                for way in (0, 1):
                    hop(base, i, 0, z, 1, way, p).start()

    def join_ring(base):
        for i in range(2):
            for p in range(PARTS):
                for way in (0, 1):
                    enter(base, i, way, p).start()

    def arrive(base, i, owner, step, way, p, forward):
        origin = lax.rem(z + step, n_sp) if way else lax.rem(z + n_sp - step, n_sp)
        hop(base, i, owner, origin, step, way, p).wait_recv()
        if forward is True:
            hop(base, i, owner, origin, step + 1, way, p).start()
        elif forward is not False:

            @pl.when(forward)
            def _():
                hop(base, i, owner, origin, step + 1, way, p).start()

        mine = held(base, i, owner, origin, p)
        home = block(weights, base + which(i), origin, p)
        if i:
            over(mine, home if base else mine, base, owner).start()
        if base and owner:
            push(mine, home, i).start()

    streams = [(i, owner, p) for i in (1, 0) for owner in (0, 1) for p in range(PARTS)]

    def carry_ring(base):
        def ring_step(step, carry):
            for i, owner, p in streams:
                arrive(base, i, owner, step, 0, p, True)
                arrive(base, i, owner, step, 1, p, step < half - 1)
            return carry

        lax.fori_loop(1, half, ring_step, 0)
        for i, owner, p in streams:
            arrive(base, i, owner, half, 0, p, False)

    def pushed():
        for i in range(2):
            ref = weights.at[RING + which(i), pl.ds(0, wrows * (n_sp - 1))]
            push(ref, ref, i).wait_recv()

    def came_over(base, owner):
        ref = weights.at[base + 2 - parity, pl.ds(0, wrows * (n_sp - 1))]
        over(ref, ref, base, owner).wait_recv()

    def pair_copy(src, dst, send, recv):
        return pltpu.make_async_remote_copy(
            src_ref=src,
            dst_ref=dst,
            send_sem=send,
            recv_sem=recv,
            device_id={"tp": partner},
            device_id_type=MESH,
        )

    def lend(k):
        src, dst = ((gap, gap_there), (shift, shift_there))[k]
        return pair_copy(src, dst, lend_send.at[k], lend_recv.at[k])

    def own_block(m):
        lines = pl.ds(pl.multiple_of(z * wrows, wrows), wrows)
        return pair_copy(
            weights.at[m, lines], others.at[m, lines], own_send.at[m], own_recv.at[m]
        )

    def hand(k):
        src = (vs_there, kf_there, kb_there, rf_there, rb_there)[k]
        dst = (vs, kf, kb, rf, rb)[k]
        return pair_copy(src, dst, hand_send.at[k], hand_recv.at[k])

    @pl.when(carrier)
    def _():
        open_ring(0)
        join_ring(RING)

    @pl.when(jnp.logical_not(carrier))
    def _():
        join_ring(0)
        open_ring(RING)
        for m in range(RING):
            own_block(m).start()

    for load in loads[6:]:
        load.wait()

    @pl.when(jnp.logical_not(carrier))
    def _():
        for k in range(2):
            lend(k).start()

    tok = tokens[...].astype(F32)
    rows = []
    for b in range(seqs):
        part = tok[:, b, :]
        scale = lax.rsqrt(jnp.mean(part * part, axis=-1, keepdims=True) + EPS)
        rows.append(part * scale * gain[...])
    tok_block = pl.ds(pl.multiple_of(here * block_rows, block_rows), block_rows)
    normed[tok_block, :] = jnp.concatenate(rows, axis=0).astype(BF16)

    def token_copy(ref, peer):
        return pltpu.make_async_remote_copy(
            src_ref=ref,
            dst_ref=ref,
            send_sem=tok_send,
            recv_sem=tok_recv,
            device_id={"tp": peer},
            device_id_type=MESH,
        )

    for d in range(1, n_tp):
        token_copy(normed.at[tok_block], lax.rem(tp + d, n_tp)).start()

    @pl.when(carrier)
    def _():
        carry_ring(0)

    rest = normed.at[pl.ds(0, block_rows * (n_tp - 1))]

    def project(matrix):
        return (
            jnp.dot(normed[...], matrix[...], preferred_element_type=F32).astype(BF16).astype(F32)
        )

    def by_sequence(ref, value):
        for t in range(n_tp):
            for b in range(seqs):
                first = spot(t) * block_rows + b * step_pos
                ref[b, t * step_pos : (t + 1) * step_pos, :] = value[
                    first : first + step_pos, :
                ]

    def silu(u):
        return u / (1.0 + jnp.exp(-u))

    at_row = lax.broadcasted_iota(jnp.int32, (span, span), 0)
    at_col = lax.broadcasted_iota(jnp.int32, (span, span), 1)
    lower = (at_row >= at_col).astype(F32)
    upper = (at_row <= at_col).astype(F32)
    def prepare(matrices, gap_ref, shift_ref, vs_ref, kf_ref, kb_ref, rf_ref, rb_ref, base):
        by_sequence(vs_ref, project(matrices[0]))

        def keys_of(d):
            key = gap_ref[d : d + 1, :] / (1.0 + jnp.exp(project(matrices[1 + d])))
            by_sequence((kf_ref, kb_ref)[d], key)

        for first in (True, False):
            if not first:
                came_over(0, 1 if base else 0)
            for d in (0, 1):

                @pl.when(parity == (d if first else 1 - d))
                def _():
                    keys_of(d)

        for b in range(seqs):
            moved = shift_ref[:, b, :]
            fwd_key, bwd_key = kf_ref[b], kb_ref[b]
            fwd_run = jnp.dot(
                lower,
                jnp.log1p(-fwd_key) + moved,
                precision=lax.Precision.HIGHEST,
                preferred_element_type=F32,
            )
            bwd_run = jnp.dot(
                upper,
                jnp.log1p(-bwd_key) + moved,
                precision=lax.Precision.HIGHEST,
                preferred_element_type=F32,
            )
            rf_ref[b] = fwd_run
            rb_ref[b] = bwd_run
            fwd_end, bwd_end = fwd_run[span - 1 : span, :], bwd_run[0:1, :]
            keys = jnp.concatenate(
                [fwd_key * jnp.exp(fwd_end - fwd_run), bwd_key * jnp.exp(bwd_end - bwd_run)],
                axis=1,
            ).astype(BF16)
            states = lax.dot_general(
                vs_ref[b].astype(BF16), keys, dims(((0,), (0,))), preferred_element_type=F32
            )
            for h in range(heads):
                c = b * heads + h
                lanes = slice(h * CH, (h + 1) * CH)
                for d, end in enumerate((fwd_end, bwd_end)):
                    local[d, base + c] = states[
                        lanes, d * width + h * CH : d * width + (h + 1) * CH
                    ].astype(BF16)
                    decay[d, base + c : base + c + 1, :] = jnp.exp(end[:, lanes])

    low_chunks = pl.ds(0, chunks)

    def give_back(d, c):
        return pair_copy(carried.at[d, c], carried.at[d, c - chunks], back_send.at[d], back_recv.at[d])

    def given_back(d):
        ref = carried.at[d, low_chunks]
        return pair_copy(ref, ref, back_send.at[d], back_recv.at[d])

    def ends(d):
        place = (n_sp - 1 - z) if d == 1 else z
        return place // BLK, lax.rem(place, BLK), (-1 if d == 1 else 1)

    def scan_copy(src, dst, send, recv, target):
        return pltpu.make_async_remote_copy(
            src_ref=src,
            dst_ref=dst,
            send_sem=send,
            recv_sem=recv,
            device_id={"sp": target},
            device_id_type=MESH,
        )

    def factor(d, way, j):
        return scan_copy(
            decay.at[d], decay_in.at[d, j - 1], d_send.at[d, j - 1], d_recv.at[d, j - 1], z + j * way
        )

    def near(d, way, c):
        return scan_copy(
            sent1.at[d, c], before.at[d, c], p1_send.at[d], p1_recv.at[d, c], z + way
        )

    def far(d, way, c):
        return scan_copy(
            sent2.at[d, c], ahead.at[d, c], p2_send.at[d, 0], p2_recv.at[d, c], z + BLK * way
        )

    def down(d, way, c):
        return scan_copy(
            sent2.at[d, c], ahead.at[d, c], p2_send.at[d, 1], p2_recv.at[d, c], z + way
        )

    def relay(d, way, c):
        return scan_copy(
            ahead.at[d, c], ahead.at[d, c], p2_send.at[d, 1], p2_recv.at[d, c], z + way
        )

    def clear():
        for d in (0, 1):
            jj, rr, way = ends(d)

            @pl.when(jj == 0)
            def _():
                ahead[d] = jnp.zeros(ahead.shape[1:], ahead.dtype)

            @pl.when(rr == 0)
            def _():
                before[d] = jnp.zeros(before.shape[1:], before.dtype)

    def exchange():
        for d in (0, 1):
            jj, rr, way = ends(d)
            for j in range(1, BLK):

                @pl.when(rr + j < BLK)
                def _():
                    factor(d, way, j).start()

    edge = (lax.rem(z, BLK) == 0) | (lax.rem(z, BLK) == BLK - 1)

    def first_step(d, c):
        jj, rr, way = ends(d)

        @pl.when(rr > 0)
        def _():
            near(d, way, c).wait_recv()

        joined = decay[d, pl.ds(c, 1), :] * before[d, c].astype(F32) + local[d, c].astype(F32)

        @pl.when(rr < BLK - 1)
        def _():
            sent1[d, c] = joined.astype(BF16)
            near(d, way, c).start()

        @pl.when(rr == BLK - 1)
        def _():
            total[d, c] = joined

            @pl.when(jj == 0)
            def _():
                sent2[d, c] = joined.astype(BF16)
                far(d, way, c).start()
                down(d, way, c).start()

    def head_start(d):
        def each(c, carry):
            first_step(d, c)
            return carry

        lax.fori_loop(0, chunks, each, 0)

    def first_pass(d, begin, lag):
        def each(turn, carry):
            @pl.when(turn < 2 * chunks)
            def _():
                first_step(d, turn)

            @pl.when(turn >= lag)
            def _():
                first_step(1 - d, turn - lag)

            return carry

        lax.fori_loop(begin, 2 * chunks + lag, each, 0)

    def factors():
        for d in (0, 1):
            jj, rr, way = ends(d)
            decay_before[d] = jnp.ones(decay_before.shape[1:], F32)
            for j in range(1, BLK):

                @pl.when(rr >= j)
                def _():
                    factor(d, way, j).wait_recv()
                    decay_before[d] = decay_before[d] * decay_in[d, j - 1]

            decay_sent[d] = decay_before[d] * decay[d]

    def second_pass(d):
        jj, rr, way = ends(d)

        def each(c, carry):
            @pl.when(jj > 0)
            def _():
                far(d, way, c).wait_recv()

            @pl.when((rr == BLK - 1) & (jj > 0) & (jj < n_blocks - 1))
            def _():
                joined = (
                    decay_sent[d, pl.ds(c, 1), :] * ahead[d, c].astype(F32) + total[d, c]
                )
                sent2[d, c] = joined.astype(BF16)
                far(d, way, c).start()
                down(d, way, c).start()

            @pl.when((rr < BLK - 2) & (jj > 0))
            def _():
                relay(d, way, c).start()

            carried[d, c] = (
                decay_before[d, pl.ds(c, 1), :] * ahead[d, c].astype(F32)
                + before[d, c].astype(F32)
            ).astype(BF16)

            @pl.when(c >= chunks)
            def _():
                give_back(d, c).start()

            return carry

        lax.fori_loop(0, 2 * chunks, each, 0)

    def inside():
        by_sequence(qs, silu(project(weights.at[5])))
        by_sequence(gs, silu(project(weights.at[4])))
        middle = span // 2 - 1
        for b in range(seqs):
            query, fwd_run, bwd_run = qs[b], rf[b], rb[b]
            fwd_mid, bwd_mid = fwd_run[middle : middle + 1, :], bwd_run[middle : middle + 1, :]
            fwd_q = (query * jnp.exp(fwd_run - fwd_mid)).astype(BF16)
            bwd_q = (query * jnp.exp(bwd_run - bwd_mid)).astype(BF16)
            fwd_k = (kf[b] * jnp.exp(fwd_mid - fwd_run)).astype(BF16)
            bwd_k = (kb[b] * jnp.exp(bwd_mid - bwd_run)).astype(BF16)
            fwd_e = (query * jnp.exp(fwd_run)).astype(BF16)
            bwd_e = (query * jnp.exp(bwd_run)).astype(BF16)
            value = vs[b].astype(BF16)
            for h in range(heads):
                c = b * heads + h
                lanes = slice(h * CH, (h + 1) * CH)
                fwd_s = lax.dot_general(
                    fwd_q[:, lanes], fwd_k[:, lanes], dims(((1,), (1,))), preferred_element_type=F32
                )
                bwd_s = lax.dot_general(
                    bwd_q[:, lanes], bwd_k[:, lanes], dims(((1,), (1,))), preferred_element_type=F32
                )
                scores = jnp.where(at_row >= at_col, fwd_s, 0.0) + jnp.where(
                    at_row <= at_col, bwd_s, 0.0
                )
                inner[c] = jnp.dot(
                    scores.astype(BF16), value[:, lanes], preferred_element_type=F32
                )
                qe[c] = jnp.concatenate([fwd_e[:, lanes], bwd_e[:, lanes]], axis=1)

    early = lax.rem(z, BLK) < BLK // 2
    low = z < half

    @pl.when(carrier)
    def _():
        clear()
        token_copy(rest, tp).wait_recv()
        prepare([weights.at[m] for m in range(RING)], gap, shift, vs, kf, kb, rf, rb, 0)

        @pl.when(early & edge)
        def _():
            head_start(0)

        @pl.when(jnp.logical_not(early) & edge)
        def _():
            head_start(1)

        for k in range(2):
            lend(k).wait_recv()
        for m in range(RING):
            own_block(m).wait_recv()
        prepare(
            [others.at[m] for m in range(RING)],
            gap_there,
            shift_there,
            vs_there,
            kf_there,
            kb_there,
            rf_there,
            rb_there,
            chunks,
        )
        exchange()
        for k in range(5):
            hand(k).start()
        begin = jnp.where(edge, chunks, 0)
        lag = jnp.where(edge, 2 * chunks, LAG)

        @pl.when(early)
        def _():
            first_pass(0, begin, lag)

        @pl.when(jnp.logical_not(early))
        def _():
            first_pass(1, begin, lag)

        factors()

        @pl.when(low)
        def _():
            second_pass(0)

        @pl.when(jnp.logical_not(low))
        def _():
            second_pass(1)

        pushed()

    @pl.when(jnp.logical_not(carrier))
    def _():
        carry_ring(RING)
        token_copy(rest, tp).wait_recv()
        for k in range(5):
            hand(k).wait_recv()

    came_over(RING, 1)
    inside()

    @pl.when(carrier)
    def _():
        @pl.when(low)
        def _():
            second_pass(1)

        @pl.when(jnp.logical_not(low))
        def _():
            second_pass(0)

    @pl.when(jnp.logical_not(carrier))
    def _():
        for d in (0, 1):
            given_back(d).wait_recv()

    for b in range(seqs):
        for h in range(heads):
            c = b * heads + h
            both = inner[c] + lax.dot_general(
                qe[c],
                jnp.concatenate([carried[0, c], carried[1, c]], axis=1),
                dims(((1,), (1,))),
                preferred_element_type=F32,
            )
            scale = lax.rsqrt(jnp.mean(both * both, axis=-1, keepdims=True) + EPS)
            gated = both * scale * head_gain[...] * gs[b, :, h * CH : (h + 1) * CH]
            for t in range(n_tp):
                first = spot(t) * block_rows + b * step_pos
                mixed[first : first + step_pos, h * CH : (h + 1) * CH] = gated[
                    t * step_pos : (t + 1) * step_pos, :
                ]

    side = n_x * block_rows

    def partial(core_index, k):
        lines = pl.ds(pl.multiple_of(core_index * side, side), side)
        return lax.dot_general(
            mixed[lines, :].astype(BF16),
            weights[3, k * (model // STRIPS) : (k + 1) * (model // STRIPS), :],
            dims(((1,), (1,))),
            preferred_element_type=F32,
        )

    strip = model // STRIPS

    def exchange_pair(k):
        columns = pl.ds(k * strip, strip)
        return pair_copy(
            given.at[:, columns], taken.at[:, columns], pair_send.at[k], pair_recv.at[k]
        )

    def piece(dest, d, k):
        lines = pl.ds(pl.multiple_of(dest * block_rows, block_rows), block_rows)
        columns = pl.ds(k * strip, strip)
        return pltpu.make_async_remote_copy(
            src_ref=summed.at[lines, columns],
            dst_ref=pieces.at[d - 1, :, columns],
            send_sem=x_send.at[d - 1, k],
            recv_sem=x_recv.at[d - 1, k],
            device_id={"tp": dest * 2 + core},
            device_id_type=MESH,
        )

    for k in range(STRIPS):
        given[:, k * strip : (k + 1) * strip] = partial(1 - core, k).astype(BF16)
        exchange_pair(k).start()
    for k in range(STRIPS):
        mine[:, k * strip : (k + 1) * strip] = partial(core, k)
    order = [2, 1, 3] if n_x == 4 else list(range(1, n_x))
    for k in range(STRIPS):
        exchange_pair(k).wait_recv()
        columns = slice(k * strip, (k + 1) * strip)
        for d in order:
            dest = lax.rem(x + d, n_x)
            lines = pl.ds(pl.multiple_of(dest * block_rows, block_rows), block_rows)
            summed[lines, columns] = (
                mine[lines, columns] + taken[lines, columns].astype(F32)
            ).astype(BF16)
            piece(dest, d, k).start()
    own_lines = pl.ds(pl.multiple_of(x * block_rows, block_rows), block_rows)
    for k in range(STRIPS):
        columns = slice(k * strip, (k + 1) * strip)
        result = mine[own_lines, columns] + taken[own_lines, columns].astype(F32)
        for d in order:
            piece(x, d, k).wait_recv()
            result = result + pieces[d - 1, :, columns].astype(F32)
        out[:, columns] = result.astype(BF16)

    def ring_left(ref, count, way, i, owner):
        lines = ref.at[0, pl.ds(0, wrows * count)]
        pltpu.make_async_remote_copy(
            src_ref=lines,
            dst_ref=lines,
            send_sem=ring_send.at[way, i, owner],
            recv_sem=ring_recv.at[way, i, owner, 0, 0],
            device_id={"sp": right},
            device_id_type=MESH,
        ).wait_send()

    for i in range(2):
        for way in (0, 1):
            ring_left(weights, half - way, way, i, 0)
            ring_left(weights, half - 1 - way, way, i, 1)
            for p in range(PARTS):
                enter(0, i, way, p).wait_send()
        lines = weights.at[0, pl.ds(0, wrows * (n_sp - 1))]
        over(lines, lines, 0, i).wait_send()
    token_copy(rest, tp).wait_send()
    @pl.when(carrier)
    def _():
        for d in (0, 1):
            jj, rr, way = ends(d)

            @pl.when(rr < BLK - 1)
            def _():
                scan_copy(sent1.at[d], before.at[d], p1_send.at[d], p1_recv.at[d, 0], z).wait_send()

            for j in range(1, BLK):

                @pl.when(rr + j < BLK)
                def _():
                    factor(d, way, j).wait_send()

            leads = (rr == BLK - 1) & (jj < n_blocks - 1)

            @pl.when(leads)
            def _():
                scan_copy(sent2.at[d], ahead.at[d], p2_send.at[d, 0], p2_recv.at[d, 0], z).wait_send()

            @pl.when(leads | ((rr < BLK - 2) & (jj > 0)))
            def _():
                scan_copy(sent2.at[d], ahead.at[d], p2_send.at[d, 1], p2_recv.at[d, 0], z).wait_send()
            given_back(d).wait_send()
        for k in range(5):
            hand(k).wait_send()

    @pl.when(jnp.logical_not(carrier))
    def _():
        for m in range(RING):
            own_block(m).wait_send()
        for k in range(2):
            lend(k).wait_send()
            lines = weights.at[0, pl.ds(0, wrows * (n_sp - 1))]
            push(lines, lines, k).wait_send()

    for k in range(STRIPS):
        exchange_pair(k).wait_send()
        for d in order:
            piece(lax.rem(x + d, n_x), d, k).wait_send()


def shards(
    n_sp,
    n_tp,
    tokens,
    norm_gain,
    w_query,
    w_value,
    w_fwd_gate,
    w_bwd_gate,
    w_out_gate,
    floor_gap,
    decay_shift,
    head_gain,
    w_out,
):
    step_pos, seqs, model = tokens.shape
    wrows, width = w_query.shape
    span = decay_shift.shape[0]
    chunks = seqs * (width // CH)
    both = 2 * chunks
    rows = step_pos * seqs
    all_rows = rows * n_tp
    n_x = n_tp // 2
    f32_rows = pltpu.VMEM((seqs, span, width), F32)
    vmem = pl.BlockSpec(memory_space=pltpu.VMEM)
    dma = pltpu.SemaphoreType.DMA
    result = pl.pallas_call(
        functools.partial(kernel, n_sp, n_tp),
        out_shape=jax.ShapeDtypeStruct((rows, model), BF16),
        in_specs=[pl.BlockSpec(memory_space=pl.ANY)] * 11,
        out_specs=vmem,
        scratch_shapes=[
            pltpu.VMEM(tokens.shape, BF16),
            pltpu.VMEM((1, model), F32),
            pltpu.VMEM((2, width), F32),
            pltpu.VMEM((span, seqs, width), F32),
            pltpu.VMEM((1, CH), F32),
            pltpu.VMEM((6, wrows * n_sp, width), BF16),
            pltpu.VMEM((RING, wrows * n_sp, width), BF16),
            pltpu.VMEM((all_rows, model), BF16),
            pltpu.VMEM((2, width), F32),
            pltpu.VMEM((span, seqs, width), F32),
            f32_rows,
            f32_rows,
            f32_rows,
            f32_rows,
            f32_rows,
            f32_rows,
            f32_rows,
            f32_rows,
            f32_rows,
            f32_rows,
            f32_rows,
            f32_rows,
            pltpu.VMEM((chunks, span, 2 * CH), BF16),
            pltpu.VMEM((chunks, span, CH), F32),
            pltpu.VMEM((2, both, CH, CH), BF16),
            pltpu.VMEM((2, both, CH), F32),
            pltpu.VMEM((2, both, CH, CH), BF16),
            pltpu.VMEM((2, BLK - 1, both, CH), F32),
            pltpu.VMEM((2, both, CH), F32),
            pltpu.VMEM((2, both, CH, CH), BF16),
            pltpu.VMEM((2, both, CH), F32),
            pltpu.VMEM((2, both, CH, CH), F32),
            pltpu.VMEM((2, both, CH, CH), BF16),
            pltpu.VMEM((2, both, CH, CH), BF16),
            pltpu.VMEM((2, both, CH, CH), BF16),
            pltpu.VMEM((all_rows, width), F32),
            pltpu.VMEM((n_x * rows, model), F32),
            pltpu.VMEM((n_x * rows, model), BF16),
            pltpu.VMEM((n_x * rows, model), BF16),
            pltpu.VMEM((n_x * rows, model), BF16),
            pltpu.VMEM((n_x - 1, rows, model), BF16),
            dma((2, 2, 2)),
            dma((2, 2, 2, n_sp // 2 + 1, PARTS)),
            dma((2, 2, PARTS)),
            dma((2,)),
            dma((2,)),
            dma((2,)),
            dma((3,)),
            dma,
            dma,
            dma((2,)),
            dma((2,)),
            dma((RING,)),
            dma((RING,)),
            dma((5,)),
            dma((5,)),
            dma((2,)),
            dma((2,)),
            dma((2, BLK - 1)),
            dma((2, BLK - 1)),
            dma((2,)),
            dma((2, both)),
            dma((2, 2)),
            dma((2, both)),
            dma((STRIPS,)),
            dma((STRIPS,)),
            dma((n_x - 1, STRIPS)),
            dma((n_x - 1, STRIPS)),
            dma((11,)),
        ],
        compiler_params=pltpu.CompilerParams(
            collective_id=0, has_side_effects=True, vmem_limit_bytes=60 * 1024 * 1024
        ),
        name="mixer",
    )(
        tokens,
        norm_gain.reshape(1, -1),
        w_query,
        w_value,
        w_fwd_gate,
        w_bwd_gate,
        w_out_gate,
        w_out.T,
        floor_gap,
        decay_shift,
        head_gain.reshape(1, -1),
    )
    return result.reshape(seqs, step_pos, model).transpose(1, 0, 2)


def solution(mesh):
    in_specs = (
        P(("sp", "tp"), "grp", None),
        P(),
        P("sp", "tp"),
        P("sp", "tp"),
        P("sp", "tp"),
        P("sp", "tp"),
        P("sp", "tp"),
        P(None, "tp"),
        P("sp", "grp", "tp"),
        P(),
        P("tp", "sp"),
    )
    return jax.shard_map(
        functools.partial(shards, mesh.shape["sp"], mesh.shape["tp"]),
        mesh=mesh,
        in_specs=in_specs,
        out_specs=P(("sp", "tp"), "grp", None),
        check_vma=False,
    )
```

```python
import functools

import jax
import jax.numpy as jnp
from jax import lax
from jax.experimental import pallas as pl
from jax.experimental.pallas import tpu as pltpu
from jax.sharding import PartitionSpec as P

MESH = pl.DeviceIdType.MESH
F32 = jnp.float32
BF16 = jnp.bfloat16
CH = 128
BLK = 4
RING = 3
CARRIER = 1
PARTS = 2
STRIPS = 2
LAG = 7
EPS = 1e-06


def dims(contract):
    return (contract, ((), ()))


def kernel(
    n_sp,
    n_tp,
    tokens_in,
    gain_in,
    w_query,
    w_value,
    w_fwd,
    w_bwd,
    w_gate,
    w_out,
    gap_in,
    shift_in,
    head_gain_in,
    out,
    tokens,
    gain,
    gap,
    shift,
    head_gain,
    weights,
    others,
    normed,
    gap_there,
    shift_there,
    vs_there,
    kf_there,
    kb_there,
    rf_there,
    rb_there,
    qs,
    vs,
    kf,
    kb,
    rf,
    rb,
    gs,
    qe,
    inner,
    local,
    decay,
    before,
    decay_in,
    decay_before,
    sent1,
    decay_sent,
    total,
    ahead,
    sent2,
    carried,
    mixed,
    mine,
    given,
    taken,
    summed,
    pieces,
    ring_send,
    ring_recv,
    first_send,
    push_send,
    push_recv,
    y_send,
    y_recv,
    tok_send,
    tok_recv,
    lend_send,
    lend_recv,
    own_send,
    own_recv,
    hand_send,
    hand_recv,
    back_send,
    back_recv,
    d_send,
    d_recv,
    p1_send,
    p1_recv,
    p2_send,
    p2_recv,
    pair_send,
    pair_recv,
    x_send,
    x_recv,
    load_sem,
):
    z = lax.axis_index("sp")
    tp = lax.axis_index("tp")
    grp = lax.axis_index("grp")
    parity = lax.rem(grp, 2)
    mate = grp + 1 - 2 * parity
    right, left = lax.rem(z + 1, n_sp), lax.rem(z + n_sp - 1, n_sp)
    n_x = n_tp // 2
    core, x = lax.rem(tp, 2), tp // 2
    partner = tp + 1 - 2 * core
    carrier = core == CARRIER
    wrows, width = w_query.shape
    step_pos, seqs, model = tokens.shape
    span = shift.shape[0]
    heads = width // CH
    chunks = seqs * heads
    n_blocks = n_sp // BLK
    block_rows = step_pos * seqs
    half = n_sp // 2

    def spot(t):
        return (t % 2) * n_x + t // 2

    here = spot(tp)

    own_rows = pl.ds(pl.multiple_of(z * wrows, wrows), wrows)
    loads = [
        (ref, weights.at[m, own_rows])
        for m, ref in enumerate((w_value, w_fwd, w_bwd, w_out, w_gate, w_query))
    ] + [
        (tokens_in, tokens),
        (gain_in, gain),
        (gap_in, gap),
        (shift_in, shift),
        (head_gain_in, head_gain),
    ]
    loads = [
        pltpu.make_async_copy(src, dst, load_sem.at[k]) for k, (src, dst) in enumerate(loads)
    ]

    barrier = pltpu.get_barrier_semaphore()
    greeted = 0
    for peer in (
        [{"sp": a, "tp": b} for a in (right, left) for b in (tp, partner)]
        + [{"tp": lax.rem(tp + d, n_tp)} for d in range(1, n_tp)]
        + [{"grp": mate, "tp": b} for b in (tp, partner)]
    ):
        pl.semaphore_signal(barrier, inc=1, device_id=peer, device_id_type=MESH)
        greeted += 1
    for load in loads:
        load.start()
    pl.semaphore_wait(barrier, greeted)
    for load in loads[:6]:
        load.wait()

    share = wrows // PARTS

    def block(ref, m, origin, p):
        return ref.at[m, pl.ds(pl.multiple_of(origin * wrows + p * share, share), share)]

    def which(i):
        return i * (1 + parity)

    def held(base, i, owner, origin, p):
        if owner:
            return block(others, which(i), origin, p)
        return block(weights, base + which(i), origin, p)

    def hop(base, i, owner, origin, step, way, p):
        ref = held(base, i, owner, origin, p)
        return pltpu.make_async_remote_copy(
            src_ref=ref,
            dst_ref=ref,
            send_sem=ring_send.at[way, i, owner],
            recv_sem=ring_recv.at[way, i, owner, step, p],
            device_id={"sp": left if way else right},
            device_id_type=MESH,
        )

    def enter(base, i, way, p):
        return pltpu.make_async_remote_copy(
            src_ref=block(weights, base + which(i), z, p),
            dst_ref=block(others, which(i), z, p),
            send_sem=first_send.at[way, i, p],
            recv_sem=ring_recv.at[way, i, 1, 1, p],
            device_id={"sp": left if way else right, "tp": partner},
            device_id_type=MESH,
        )

    def push(src, dst, i):
        return pltpu.make_async_remote_copy(
            src_ref=src,
            dst_ref=dst,
            send_sem=push_send.at[i],
            recv_sem=push_recv.at[i],
            device_id={"tp": partner},
            device_id_type=MESH,
        )

    def over(src, dst, base, owner):
        return pltpu.make_async_remote_copy(
            src_ref=src,
            dst_ref=dst,
            send_sem=y_send.at[owner],
            recv_sem=y_recv.at[2 if base else owner],
            device_id={"grp": mate, "tp": partner if base and owner else tp},
            device_id_type=MESH,
        )

    def open_ring(base):
        for i in range(2):
            for p in range(PARTS):
                for way in (0, 1):
                    hop(base, i, 0, z, 1, way, p).start()

    def join_ring(base):
        for i in range(2):
            for p in range(PARTS):
                for way in (0, 1):
                    enter(base, i, way, p).start()

    def arrive(base, i, owner, step, way, p, forward):
        origin = lax.rem(z + step, n_sp) if way else lax.rem(z + n_sp - step, n_sp)
        hop(base, i, owner, origin, step, way, p).wait_recv()
        if forward is True:
            hop(base, i, owner, origin, step + 1, way, p).start()
        elif forward is not False:

            @pl.when(forward)
            def _():
                hop(base, i, owner, origin, step + 1, way, p).start()

        mine = held(base, i, owner, origin, p)
        home = block(weights, base + which(i), origin, p)
        if i:
            over(mine, home if base else mine, base, owner).start()
        if base and owner:
            push(mine, home, i).start()

    streams = [(i, owner, p) for i in (1, 0) for owner in (0, 1) for p in range(PARTS)]

    def carry_ring(base):
        def ring_step(step, carry):
            for i, owner, p in streams:
                arrive(base, i, owner, step, 0, p, True)
                arrive(base, i, owner, step, 1, p, step < half - 1)
            return carry

        lax.fori_loop(1, half, ring_step, 0)
        for i, owner, p in streams:
            arrive(base, i, owner, half, 0, p, False)

    def pushed():
        for i in range(2):
            ref = weights.at[RING + which(i), pl.ds(0, wrows * (n_sp - 1))]
            push(ref, ref, i).wait_recv()

    def came_over(base, owner):
        ref = weights.at[base + 2 - parity, pl.ds(0, wrows * (n_sp - 1))]
        over(ref, ref, base, owner).wait_recv()

    def pair_copy(src, dst, send, recv):
        return pltpu.make_async_remote_copy(
            src_ref=src,
            dst_ref=dst,
            send_sem=send,
            recv_sem=recv,
            device_id={"tp": partner},
            device_id_type=MESH,
        )

    def lend(k):
        src, dst = ((gap, gap_there), (shift, shift_there))[k]
        return pair_copy(src, dst, lend_send.at[k], lend_recv.at[k])

    def own_block(m):
        lines = pl.ds(pl.multiple_of(z * wrows, wrows), wrows)
        return pair_copy(
            weights.at[m, lines], others.at[m, lines], own_send.at[m], own_recv.at[m]
        )

    def hand(k):
        src = (vs_there, kf_there, kb_there, rf_there, rb_there)[k]
        dst = (vs, kf, kb, rf, rb)[k]
        return pair_copy(src, dst, hand_send.at[k], hand_recv.at[k])

    @pl.when(carrier)
    def _():
        open_ring(0)
        join_ring(RING)

    @pl.when(jnp.logical_not(carrier))
    def _():
        join_ring(0)
        open_ring(RING)
        for m in range(RING):
            own_block(m).start()

    for load in loads[6:]:
        load.wait()

    @pl.when(jnp.logical_not(carrier))
    def _():
        for k in range(2):
            lend(k).start()

    tok = tokens[...].astype(F32)
    rows = []
    for b in range(seqs):
        part = tok[:, b, :]
        scale = lax.rsqrt(jnp.mean(part * part, axis=-1, keepdims=True) + EPS)
        rows.append(part * scale * gain[...])
    tok_block = pl.ds(pl.multiple_of(here * block_rows, block_rows), block_rows)
    normed[tok_block, :] = jnp.concatenate(rows, axis=0).astype(BF16)

    def token_copy(ref, peer):
        return pltpu.make_async_remote_copy(
            src_ref=ref,
            dst_ref=ref,
            send_sem=tok_send,
            recv_sem=tok_recv,
            device_id={"tp": peer},
            device_id_type=MESH,
        )

    for d in range(1, n_tp):
        token_copy(normed.at[tok_block], lax.rem(tp + d, n_tp)).start()

    @pl.when(carrier)
    def _():
        carry_ring(0)

    rest = normed.at[pl.ds(0, block_rows * (n_tp - 1))]

    def project(matrix):
        return (
            jnp.dot(normed[...], matrix[...], preferred_element_type=F32).astype(BF16).astype(F32)
        )

    def by_sequence(ref, value):
        for t in range(n_tp):
            for b in range(seqs):
                first = spot(t) * block_rows + b * step_pos
                ref[b, t * step_pos : (t + 1) * step_pos, :] = value[
                    first : first + step_pos, :
                ]

    def silu(u):
        return u / (1.0 + jnp.exp(-u))

    at_row = lax.broadcasted_iota(jnp.int32, (span, span), 0)
    at_col = lax.broadcasted_iota(jnp.int32, (span, span), 1)
    lower = (at_row >= at_col).astype(F32)
    upper = (at_row <= at_col).astype(F32)
    def prepare(matrices, gap_ref, shift_ref, vs_ref, kf_ref, kb_ref, rf_ref, rb_ref, base):
        by_sequence(vs_ref, project(matrices[0]))

        def keys_of(d):
            key = gap_ref[d : d + 1, :] / (1.0 + jnp.exp(project(matrices[1 + d])))
            by_sequence((kf_ref, kb_ref)[d], key)

        for first in (True, False):
            if not first:
                came_over(0, 1 if base else 0)
            for d in (0, 1):

                @pl.when(parity == (d if first else 1 - d))
                def _():
                    keys_of(d)

        for b in range(seqs):
            moved = shift_ref[:, b, :]
            fwd_key, bwd_key = kf_ref[b], kb_ref[b]
            fwd_run = jnp.dot(
                lower,
                jnp.log1p(-fwd_key) + moved,
                precision=lax.Precision.HIGHEST,
                preferred_element_type=F32,
            )
            bwd_run = jnp.dot(
                upper,
                jnp.log1p(-bwd_key) + moved,
                precision=lax.Precision.HIGHEST,
                preferred_element_type=F32,
            )
            rf_ref[b] = fwd_run
            rb_ref[b] = bwd_run
            fwd_end, bwd_end = fwd_run[span - 1 : span, :], bwd_run[0:1, :]
            keys = jnp.concatenate(
                [fwd_key * jnp.exp(fwd_end - fwd_run), bwd_key * jnp.exp(bwd_end - bwd_run)],
                axis=1,
            ).astype(BF16)
            states = lax.dot_general(
                vs_ref[b].astype(BF16), keys, dims(((0,), (0,))), preferred_element_type=F32
            )
            for h in range(heads):
                c = b * heads + h
                lanes = slice(h * CH, (h + 1) * CH)
                for d, end in enumerate((fwd_end, bwd_end)):
                    local[d, base + c] = states[
                        lanes, d * width + h * CH : d * width + (h + 1) * CH
                    ].astype(BF16)
                    decay[d, base + c : base + c + 1, :] = jnp.exp(end[:, lanes])

    low_chunks = pl.ds(0, chunks)

    def give_back(d, c):
        return pair_copy(carried.at[d, c], carried.at[d, c - chunks], back_send.at[d], back_recv.at[d])

    def given_back(d):
        ref = carried.at[d, low_chunks]
        return pair_copy(ref, ref, back_send.at[d], back_recv.at[d])

    def ends(d):
        place = (n_sp - 1 - z) if d == 1 else z
        return place // BLK, lax.rem(place, BLK), (-1 if d == 1 else 1)

    def scan_copy(src, dst, send, recv, target):
        return pltpu.make_async_remote_copy(
            src_ref=src,
            dst_ref=dst,
            send_sem=send,
            recv_sem=recv,
            device_id={"sp": target},
            device_id_type=MESH,
        )

    def factor(d, way, j):
        return scan_copy(
            decay.at[d], decay_in.at[d, j - 1], d_send.at[d, j - 1], d_recv.at[d, j - 1], z + j * way
        )

    def near(d, way, c):
        return scan_copy(
            sent1.at[d, c], before.at[d, c], p1_send.at[d], p1_recv.at[d, c], z + way
        )

    def far(d, way, c):
        return scan_copy(
            sent2.at[d, c], ahead.at[d, c], p2_send.at[d, 0], p2_recv.at[d, c], z + BLK * way
        )

    def down(d, way, c):
        return scan_copy(
            sent2.at[d, c], ahead.at[d, c], p2_send.at[d, 1], p2_recv.at[d, c], z + way
        )

    def relay(d, way, c):
        return scan_copy(
            ahead.at[d, c], ahead.at[d, c], p2_send.at[d, 1], p2_recv.at[d, c], z + way
        )

    def clear():
        for d in (0, 1):
            jj, rr, way = ends(d)

            @pl.when(jj == 0)
            def _():
                ahead[d] = jnp.zeros(ahead.shape[1:], ahead.dtype)

            @pl.when(rr == 0)
            def _():
                before[d] = jnp.zeros(before.shape[1:], before.dtype)

    def exchange():
        for d in (0, 1):
            jj, rr, way = ends(d)
            for j in range(1, BLK):

                @pl.when(rr + j < BLK)
                def _():
                    factor(d, way, j).start()

    edge = (lax.rem(z, BLK) == 0) | (lax.rem(z, BLK) == BLK - 1)

    def first_step(d, c):
        jj, rr, way = ends(d)

        @pl.when(rr > 0)
        def _():
            near(d, way, c).wait_recv()

        joined = decay[d, pl.ds(c, 1), :] * before[d, c].astype(F32) + local[d, c].astype(F32)

        @pl.when(rr < BLK - 1)
        def _():
            sent1[d, c] = joined.astype(BF16)
            near(d, way, c).start()

        @pl.when(rr == BLK - 1)
        def _():
            total[d, c] = joined

            @pl.when(jj == 0)
            def _():
                sent2[d, c] = joined.astype(BF16)
                far(d, way, c).start()
                down(d, way, c).start()

    def head_start(d):
        def each(c, carry):
            first_step(d, c)
            return carry

        lax.fori_loop(0, chunks, each, 0)

    def first_pass(d, begin, lag):
        def each(turn, carry):
            @pl.when(turn < 2 * chunks)
            def _():
                first_step(d, turn)

            @pl.when(turn >= lag)
            def _():
                first_step(1 - d, turn - lag)

            return carry

        lax.fori_loop(begin, 2 * chunks + lag, each, 0)

    def factors():
        for d in (0, 1):
            jj, rr, way = ends(d)
            decay_before[d] = jnp.ones(decay_before.shape[1:], F32)
            for j in range(1, BLK):

                @pl.when(rr >= j)
                def _():
                    factor(d, way, j).wait_recv()
                    decay_before[d] = decay_before[d] * decay_in[d, j - 1]

            decay_sent[d] = decay_before[d] * decay[d]

    def second_pass(d):
        jj, rr, way = ends(d)

        def each(c, carry):
            @pl.when(jj > 0)
            def _():
                far(d, way, c).wait_recv()

            @pl.when((rr == BLK - 1) & (jj > 0) & (jj < n_blocks - 1))
            def _():
                joined = (
                    decay_sent[d, pl.ds(c, 1), :] * ahead[d, c].astype(F32) + total[d, c]
                )
                sent2[d, c] = joined.astype(BF16)
                far(d, way, c).start()
                down(d, way, c).start()

            @pl.when((rr < BLK - 2) & (jj > 0))
            def _():
                relay(d, way, c).start()

            carried[d, c] = (
                decay_before[d, pl.ds(c, 1), :] * ahead[d, c].astype(F32)
                + before[d, c].astype(F32)
            ).astype(BF16)

            @pl.when(c >= chunks)
            def _():
                give_back(d, c).start()

            return carry

        lax.fori_loop(0, 2 * chunks, each, 0)

    def inside():
        by_sequence(qs, silu(project(weights.at[5])))
        by_sequence(gs, silu(project(weights.at[4])))
        middle = span // 2 - 1
        for b in range(seqs):
            query, fwd_run, bwd_run = qs[b], rf[b], rb[b]
            fwd_mid, bwd_mid = fwd_run[middle : middle + 1, :], bwd_run[middle : middle + 1, :]
            fwd_q = (query * jnp.exp(fwd_run - fwd_mid)).astype(BF16)
            bwd_q = (query * jnp.exp(bwd_run - bwd_mid)).astype(BF16)
            fwd_k = (kf[b] * jnp.exp(fwd_mid - fwd_run)).astype(BF16)
            bwd_k = (kb[b] * jnp.exp(bwd_mid - bwd_run)).astype(BF16)
            fwd_e = (query * jnp.exp(fwd_run)).astype(BF16)
            bwd_e = (query * jnp.exp(bwd_run)).astype(BF16)
            value = vs[b].astype(BF16)
            for h in range(heads):
                c = b * heads + h
                lanes = slice(h * CH, (h + 1) * CH)
                fwd_s = lax.dot_general(
                    fwd_q[:, lanes], fwd_k[:, lanes], dims(((1,), (1,))), preferred_element_type=F32
                )
                bwd_s = lax.dot_general(
                    bwd_q[:, lanes], bwd_k[:, lanes], dims(((1,), (1,))), preferred_element_type=F32
                )
                scores = jnp.where(at_row >= at_col, fwd_s, 0.0) + jnp.where(
                    at_row <= at_col, bwd_s, 0.0
                )
                inner[c] = jnp.dot(
                    scores.astype(BF16), value[:, lanes], preferred_element_type=F32
                )
                qe[c] = jnp.concatenate([fwd_e[:, lanes], bwd_e[:, lanes]], axis=1)

    early = lax.rem(z, BLK) < BLK // 2
    near_end = jnp.where(z < half, z, n_sp - 1 - z)
    waits = near_end // BLK > 0
    leads_other = (near_end // BLK == n_blocks // 2 - 1) & (lax.rem(near_end, BLK) == 0)
    low = (z < half) != leads_other

    @pl.when(carrier)
    def _():
        clear()
        token_copy(rest, tp).wait_recv()
        prepare([weights.at[m] for m in range(RING)], gap, shift, vs, kf, kb, rf, rb, 0)

        @pl.when(early & edge)
        def _():
            head_start(0)

        @pl.when(jnp.logical_not(early) & edge)
        def _():
            head_start(1)

        for k in range(2):
            lend(k).wait_recv()
        for m in range(RING):
            own_block(m).wait_recv()
        prepare(
            [others.at[m] for m in range(RING)],
            gap_there,
            shift_there,
            vs_there,
            kf_there,
            kb_there,
            rf_there,
            rb_there,
            chunks,
        )
        exchange()
        for k in range(5):
            hand(k).start()
        begin = jnp.where(edge, chunks, 0)
        lag = jnp.where(edge, 2 * chunks, LAG)

        @pl.when(early)
        def _():
            first_pass(0, begin, lag)

        @pl.when(jnp.logical_not(early))
        def _():
            first_pass(1, begin, lag)

        factors()

        def own_part():
            pushed()
            came_over(RING, 1)
            inside()

        @pl.when(waits)
        def _():
            own_part()

        @pl.when(low)
        def _():
            second_pass(0)

        @pl.when(jnp.logical_not(low))
        def _():
            second_pass(1)

        @pl.when(jnp.logical_not(waits))
        def _():
            own_part()

    @pl.when(jnp.logical_not(carrier))
    def _():
        carry_ring(RING)
        token_copy(rest, tp).wait_recv()
        for k in range(5):
            hand(k).wait_recv()
        came_over(RING, 1)
        inside()

    @pl.when(carrier)
    def _():
        @pl.when(low)
        def _():
            second_pass(1)

        @pl.when(jnp.logical_not(low))
        def _():
            second_pass(0)

    @pl.when(jnp.logical_not(carrier))
    def _():
        for d in (0, 1):
            given_back(d).wait_recv()

    for b in range(seqs):
        for h in range(heads):
            c = b * heads + h
            both = inner[c] + lax.dot_general(
                qe[c],
                jnp.concatenate([carried[0, c], carried[1, c]], axis=1),
                dims(((1,), (1,))),
                preferred_element_type=F32,
            )
            scale = lax.rsqrt(jnp.mean(both * both, axis=-1, keepdims=True) + EPS)
            gated = both * scale * head_gain[...] * gs[b, :, h * CH : (h + 1) * CH]
            for t in range(n_tp):
                first = spot(t) * block_rows + b * step_pos
                mixed[first : first + step_pos, h * CH : (h + 1) * CH] = gated[
                    t * step_pos : (t + 1) * step_pos, :
                ]

    side = n_x * block_rows

    def partial(core_index, k):
        lines = pl.ds(pl.multiple_of(core_index * side, side), side)
        return lax.dot_general(
            mixed[lines, :].astype(BF16),
            weights[3, k * (model // STRIPS) : (k + 1) * (model // STRIPS), :],
            dims(((1,), (1,))),
            preferred_element_type=F32,
        )

    strip = model // STRIPS

    def exchange_pair(k):
        columns = pl.ds(k * strip, strip)
        return pair_copy(
            given.at[:, columns], taken.at[:, columns], pair_send.at[k], pair_recv.at[k]
        )

    def piece(dest, d, k):
        lines = pl.ds(pl.multiple_of(dest * block_rows, block_rows), block_rows)
        columns = pl.ds(k * strip, strip)
        return pltpu.make_async_remote_copy(
            src_ref=summed.at[lines, columns],
            dst_ref=pieces.at[d - 1, :, columns],
            send_sem=x_send.at[d - 1, k],
            recv_sem=x_recv.at[d - 1, k],
            device_id={"tp": dest * 2 + core},
            device_id_type=MESH,
        )

    for k in range(STRIPS):
        given[:, k * strip : (k + 1) * strip] = partial(1 - core, k).astype(BF16)
        exchange_pair(k).start()
    for k in range(STRIPS):
        mine[:, k * strip : (k + 1) * strip] = partial(core, k)
    order = [2, 1, 3] if n_x == 4 else list(range(1, n_x))
    for k in range(STRIPS):
        exchange_pair(k).wait_recv()
        columns = slice(k * strip, (k + 1) * strip)
        for d in order:
            dest = lax.rem(x + d, n_x)
            lines = pl.ds(pl.multiple_of(dest * block_rows, block_rows), block_rows)
            summed[lines, columns] = (
                mine[lines, columns] + taken[lines, columns].astype(F32)
            ).astype(BF16)
            piece(dest, d, k).start()
    own_lines = pl.ds(pl.multiple_of(x * block_rows, block_rows), block_rows)
    for k in range(STRIPS):
        columns = slice(k * strip, (k + 1) * strip)
        result = mine[own_lines, columns] + taken[own_lines, columns].astype(F32)
        for d in order:
            piece(x, d, k).wait_recv()
            result = result + pieces[d - 1, :, columns].astype(F32)
        out[:, columns] = result.astype(BF16)

    def ring_left(ref, count, way, i, owner):
        lines = ref.at[0, pl.ds(0, wrows * count)]
        pltpu.make_async_remote_copy(
            src_ref=lines,
            dst_ref=lines,
            send_sem=ring_send.at[way, i, owner],
            recv_sem=ring_recv.at[way, i, owner, 0, 0],
            device_id={"sp": right},
            device_id_type=MESH,
        ).wait_send()

    for i in range(2):
        for way in (0, 1):
            ring_left(weights, half - way, way, i, 0)
            ring_left(weights, half - 1 - way, way, i, 1)
            for p in range(PARTS):
                enter(0, i, way, p).wait_send()
        lines = weights.at[0, pl.ds(0, wrows * (n_sp - 1))]
        over(lines, lines, 0, i).wait_send()
    token_copy(rest, tp).wait_send()
    @pl.when(carrier)
    def _():
        for d in (0, 1):
            jj, rr, way = ends(d)

            @pl.when(rr < BLK - 1)
            def _():
                scan_copy(sent1.at[d], before.at[d], p1_send.at[d], p1_recv.at[d, 0], z).wait_send()

            for j in range(1, BLK):

                @pl.when(rr + j < BLK)
                def _():
                    factor(d, way, j).wait_send()

            leads = (rr == BLK - 1) & (jj < n_blocks - 1)

            @pl.when(leads)
            def _():
                scan_copy(sent2.at[d], ahead.at[d], p2_send.at[d, 0], p2_recv.at[d, 0], z).wait_send()

            @pl.when(leads | ((rr < BLK - 2) & (jj > 0)))
            def _():
                scan_copy(sent2.at[d], ahead.at[d], p2_send.at[d, 1], p2_recv.at[d, 0], z).wait_send()
            given_back(d).wait_send()
        for k in range(5):
            hand(k).wait_send()

    @pl.when(jnp.logical_not(carrier))
    def _():
        for m in range(RING):
            own_block(m).wait_send()
        for k in range(2):
            lend(k).wait_send()
            lines = weights.at[0, pl.ds(0, wrows * (n_sp - 1))]
            push(lines, lines, k).wait_send()

    for k in range(STRIPS):
        exchange_pair(k).wait_send()
        for d in order:
            piece(lax.rem(x + d, n_x), d, k).wait_send()


def shards(
    n_sp,
    n_tp,
    tokens,
    norm_gain,
    w_query,
    w_value,
    w_fwd_gate,
    w_bwd_gate,
    w_out_gate,
    floor_gap,
    decay_shift,
    head_gain,
    w_out,
):
    step_pos, seqs, model = tokens.shape
    wrows, width = w_query.shape
    span = decay_shift.shape[0]
    chunks = seqs * (width // CH)
    both = 2 * chunks
    rows = step_pos * seqs
    all_rows = rows * n_tp
    n_x = n_tp // 2
    f32_rows = pltpu.VMEM((seqs, span, width), F32)
    vmem = pl.BlockSpec(memory_space=pltpu.VMEM)
    dma = pltpu.SemaphoreType.DMA
    result = pl.pallas_call(
        functools.partial(kernel, n_sp, n_tp),
        out_shape=jax.ShapeDtypeStruct((rows, model), BF16),
        in_specs=[pl.BlockSpec(memory_space=pl.ANY)] * 11,
        out_specs=vmem,
        scratch_shapes=[
            pltpu.VMEM(tokens.shape, BF16),
            pltpu.VMEM((1, model), F32),
            pltpu.VMEM((2, width), F32),
            pltpu.VMEM((span, seqs, width), F32),
            pltpu.VMEM((1, CH), F32),
            pltpu.VMEM((6, wrows * n_sp, width), BF16),
            pltpu.VMEM((RING, wrows * n_sp, width), BF16),
            pltpu.VMEM((all_rows, model), BF16),
            pltpu.VMEM((2, width), F32),
            pltpu.VMEM((span, seqs, width), F32),
            f32_rows,
            f32_rows,
            f32_rows,
            f32_rows,
            f32_rows,
            f32_rows,
            f32_rows,
            f32_rows,
            f32_rows,
            f32_rows,
            f32_rows,
            f32_rows,
            pltpu.VMEM((chunks, span, 2 * CH), BF16),
            pltpu.VMEM((chunks, span, CH), F32),
            pltpu.VMEM((2, both, CH, CH), BF16),
            pltpu.VMEM((2, both, CH), F32),
            pltpu.VMEM((2, both, CH, CH), BF16),
            pltpu.VMEM((2, BLK - 1, both, CH), F32),
            pltpu.VMEM((2, both, CH), F32),
            pltpu.VMEM((2, both, CH, CH), BF16),
            pltpu.VMEM((2, both, CH), F32),
            pltpu.VMEM((2, both, CH, CH), F32),
            pltpu.VMEM((2, both, CH, CH), BF16),
            pltpu.VMEM((2, both, CH, CH), BF16),
            pltpu.VMEM((2, both, CH, CH), BF16),
            pltpu.VMEM((all_rows, width), F32),
            pltpu.VMEM((n_x * rows, model), F32),
            pltpu.VMEM((n_x * rows, model), BF16),
            pltpu.VMEM((n_x * rows, model), BF16),
            pltpu.VMEM((n_x * rows, model), BF16),
            pltpu.VMEM((n_x - 1, rows, model), BF16),
            dma((2, 2, 2)),
            dma((2, 2, 2, n_sp // 2 + 1, PARTS)),
            dma((2, 2, PARTS)),
            dma((2,)),
            dma((2,)),
            dma((2,)),
            dma((3,)),
            dma,
            dma,
            dma((2,)),
            dma((2,)),
            dma((RING,)),
            dma((RING,)),
            dma((5,)),
            dma((5,)),
            dma((2,)),
            dma((2,)),
            dma((2, BLK - 1)),
            dma((2, BLK - 1)),
            dma((2,)),
            dma((2, both)),
            dma((2, 2)),
            dma((2, both)),
            dma((STRIPS,)),
            dma((STRIPS,)),
            dma((n_x - 1, STRIPS)),
            dma((n_x - 1, STRIPS)),
            dma((11,)),
        ],
        compiler_params=pltpu.CompilerParams(
            collective_id=0, has_side_effects=True, vmem_limit_bytes=60 * 1024 * 1024
        ),
        name="mixer",
    )(
        tokens,
        norm_gain.reshape(1, -1),
        w_query,
        w_value,
        w_fwd_gate,
        w_bwd_gate,
        w_out_gate,
        w_out.T,
        floor_gap,
        decay_shift,
        head_gain.reshape(1, -1),
    )
    return result.reshape(seqs, step_pos, model).transpose(1, 0, 2)


def solution(mesh):
    in_specs = (
        P(("sp", "tp"), "grp", None),
        P(),
        P("sp", "tp"),
        P("sp", "tp"),
        P("sp", "tp"),
        P("sp", "tp"),
        P("sp", "tp"),
        P(None, "tp"),
        P("sp", "grp", "tp"),
        P(),
        P("tp", "sp"),
    )
    return jax.shard_map(
        functools.partial(shards, mesh.shape["sp"], mesh.shape["tp"]),
        mesh=mesh,
        in_specs=in_specs,
        out_specs=P(("sp", "tp"), "grp", None),
        check_vma=False,
    )
```
